32 devices in a mesh: st: 8 (over z, y), tp: 4 (over x, core).
Axes of the slice: x: 2, y: 2, z: 4, core: 2. Of those that a mesh axis runs over, the one named last changes fastest.
Arguments:
- queries: bfloat16 [8192, 1024], P('st', 'tp'), may hold values from -540 to 540
- gate_pre: bfloat16 [8192, 1024], P('st', 'tp'), may hold values from -6 to 6
- cotangent: bfloat16 [8192, 1024], P('st', 'tp'), may hold values from -6 to 6
- store: bfloat16 [10240, 2048], P('st'), may hold values from -6 to 6
- store_gain: float32 [2048], replicated, may hold values from 0.1 to 1.9
- w_key: bfloat16 [2048, 1024], P(None, 'tp'), may hold values from -0.125 to 0.125
- w_value: bfloat16 [2048, 1024], P(None, 'tp'), may hold values from -0.125 to 0.125
- owners: int32 [64, 4], P('st'), may hold values from 0 to 7, all different within a row; in each aligned block of 8 rows (0 to 7, 8 to 15, ...) at most 8 rows name the same one
- slots: int32 [64, 4], P('st'), may hold values from 0 to 19
Outputs:
- grad_queries: float32 [8192, 1024], P('st', 'tp')
- grad_store: float32 [10240, 2048], P(('st', 'tp'))
- grad_w_value: float32 [2048, 1024], P('st', 'tp')
The draws below stay inside these ranges and needn't reach their ends.
Inputs may be any that keep to these rules, and one draw needn't show every extreme that they name: Each block names 4 different owners. Among the blocks of one device no owner is named twice.
All inputs are finite; a program needn't handle non-finite values.
Results may differ from the reference program's by a relative error of at most 0.014.
Values may be sent and summed in bfloat16 or wider, within the bound.
A program may use at most 192 MiB of HBM per device.

```python
import math
import jax
import jax.numpy as jnp
import numpy as np
from jax import lax

D = 2048
HEADS = 8
HD = 128
PLEN = 64
BLK = 128
NPB = 4
PASS_DEV = 20
XW = 1024
BLK_DEV = 8
CAP = 8
TOKENS = 8192
BLOCKS = 64
PASSAGES = 160
ROWS = 10240
N_ST = 8


def draw_queries(key, part):
    first_key = jax.random.fold_in(key, 11)
    drawn = jnp.clip(jax.random.normal(first_key, (TOKENS, XW), jnp.float32), -6.0, 6.0)
    return drawn.astype(jnp.bfloat16)


def draw_cotangent(key, part):
    first_key = jax.random.fold_in(key, 13)
    drawn = jnp.clip(jax.random.normal(first_key, (TOKENS, XW), jnp.float32), -6.0, 6.0)
    return drawn.astype(jnp.bfloat16)


def set_ends(array, stream_key, least, high):
    place = [jax.random.randint(jax.random.fold_in(stream_key, axis), (), 0, length) for axis, length in enumerate(array.shape)]
    widest = array.shape.index(max(array.shape))
    neighbour = place[:widest] + [(place[widest] + 1) % array.shape[widest]] + place[widest + 1:]
    return array.at[tuple(place)].set(least).at[tuple(neighbour)].set(high)


def shard_levels(key, extent, shards, low, largest):
    gain = 1.0
    for position, shards_of in shards:
        heights = jax.random.uniform(jax.random.fold_in(jax.random.fold_in(key, 6), position), (shards_of,), jnp.float32, low / len(shards), largest / len(shards))
        gain = gain * jnp.repeat(jnp.exp(heights), extent[position] // shards_of).reshape((-1,) + (1,) * (len(extent) - 1 - position))
    return gain


def rank_bounds(number_of, skew):
    portions = [(1 << 20) // math.isqrt(grade ** skew) + 1 for grade in range(1, number_of + 1)]
    width = 1 + sum(portions) // (1 << 30)
    return np.cumsum(np.array([max(1, weight // width) for weight in portions]))


def ranked_ids(rng, dims, count, skew):
    table = rank_bounds(count, skew)
    lot = jax.random.randint(jax.random.fold_in(rng, 1), dims, 0, int(table[count - 1]))
    standing = jnp.searchsorted(jnp.asarray(table, jnp.int32), lot, side="right")
    return jax.random.permutation(jax.random.fold_in(rng, 2), count)[standing].astype(jnp.int32)


def routed_block(own_key, own, number, rows, count, top, bound, lean):
    sequence = jax.random.permutation(own_key, count)
    heavy_load, common = portions_of(count, rows * top, bound, lean, True), portions_of(count, rows * top, bound, lean, False)
    places = jnp.arange(count)

    def named(lengths, rotation):
        used = int((lengths > 0).sum())
        fixed = max(1, used // 4)
        moved = fixed + (places - fixed + rotation * (used - fixed)) % max(1, count - fixed)
        return jnp.zeros((count,), jnp.int32).at[sequence[jnp.where(places < fixed, places, moved)]].set(jnp.asarray(lengths, jnp.int32))

    lengths = jnp.where(number % 4 == 0, named(heavy_load, number // 4), named(common, number - number // 4 - 1))
    mixed = jax.random.permutation(jax.random.fold_in(own, 3), count)
    giver, sink = mixed[0:count // 2 * 2:2], mixed[1:count // 2 * 2:2]
    room = jnp.minimum(lengths[giver] - 1, bound - lengths[sink]) // 2
    room = jnp.where((giver == sequence[0]) | (sink == sequence[0]) | (lengths[sink] == 0), 0, jnp.maximum(room, 0))
    moved = jax.random.randint(jax.random.fold_in(own, 4), (count // 2,), 0, 1 << 20) % (room + 1)
    lengths = lengths.at[giver].add(-moved).at[sink].add(moved)
    labels = jnp.searchsorted(jnp.cumsum(lengths), jnp.arange(rows * top), side="right").astype(jnp.int32)
    listing = labels.reshape(top, rows).T
    listing = listing[jax.random.permutation(jax.random.fold_in(own, 1), rows)]
    rotation = jax.random.randint(jax.random.fold_in(own, 2), (rows, 1), 0, top)
    return jnp.take_along_axis(listing, (jnp.arange(top)[None, :] + rotation) % top, axis=1)


def portions_of(amount, total, bound, slope, full):
    weights = [(1 << 20) // math.isqrt(rank ** slope) + 1 for rank in range(1, amount + 1)]
    largest = bound if full else min(bound, max(-(-total // amount), total * weights[0] // sum(weights)))
    least = 1 if total - largest >= amount - 1 else 0
    counts, surplus = [largest] + [least] * (amount - 1), total - largest - least * (amount - 1)
    while surplus > 0:
        movable = [i for i in range(1, amount) if counts[i] < largest] or [i for i in range(1, amount) if counts[i] < bound]
        whole, budget = sum([weights[i] for i in movable]), surplus
        for i in movable:
            addition = min(bound - counts[i], max(1, budget * weights[i] // whole), surplus)
            counts[i] = counts[i] + addition
            surplus = surplus - addition
    return np.array(counts)


def normal_values(own_key, dims, scale, bound, split=(), kind=jnp.bfloat16):
    factor_of = shard_levels(own_key, dims, split, -0.22, 0.18) if split else 1.0
    values = jax.random.normal(own_key, dims, jnp.float32) * scale * factor_of
    return jnp.minimum(jnp.maximum(values, -bound), bound).astype(kind)


def setup_inputs(seed: int = 0) -> dict:
    key_of = jax.random.split(jax.random.key(seed), 10)
    queries = draw_queries(jax.random.fold_in(key_of[9], 71), 0)
    gate_pre = normal_values(key_of[1], (TOKENS, XW), 1.5, 6.0, ((0, 8), (1, 4)))
    cotangent = draw_cotangent(jax.random.fold_in(key_of[9], 71), 0)
    store = normal_values(key_of[3], (ROWS, D), 1.0, 6.0, ((0, 8),))
    store_gain = jnp.clip(1.0 + 0.18 * jax.random.normal(key_of[4], (D,), jnp.float32), 0.1, 1.9)
    w_key = normal_values(key_of[5], (D, XW), D ** -0.5, 0.125, ((1, 4),))
    w_value = normal_values(key_of[6], (D, XW), D ** -0.5, 0.125, ((1, 4),))
    owners_keys = jax.random.split(jax.random.fold_in(key_of[7], 1), BLOCKS // BLK_DEV)
    owners_turns = jax.random.permutation(jax.random.fold_in(key_of[7], 3), BLOCKS // BLK_DEV)
    owners = jax.vmap(lambda own, number: routed_block(jax.random.fold_in(key_of[7], 2), own, number, BLK_DEV, N_ST, NPB, CAP, 2))(owners_keys, owners_turns).reshape((BLOCKS, NPB))
    slots = set_ends(ranked_ids(key_of[8], (BLOCKS, NPB), PASS_DEV, 2), jax.random.fold_in(key_of[8], 3), 0, PASS_DEV - 1).astype(jnp.int32)
    return {"queries": queries, "gate_pre": gate_pre, "cotangent": cotangent, "store": store, "store_gain": store_gain, "w_key": w_key, "w_value": w_value, "owners": owners, "slots": slots}


EPS = 1e-06

def reference(queries, gate_pre, cotangent, store, store_gain, w_key, w_value, owners, slots):
    store_rows = store.astype(jnp.float32)
    row_inverse = lax.rsqrt(lax.optimization_barrier(jnp.mean(store_rows * store_rows, axis=-1, keepdims=True)) + EPS)
    normed = (store_rows * row_inverse * store_gain).astype(jnp.bfloat16)
    key_table = jnp.dot(normed, w_key, preferred_element_type=jnp.float32).astype(jnp.bfloat16).reshape(PASSAGES, PLEN, XW)
    value_table = jnp.dot(normed, w_value, preferred_element_type=jnp.float32).astype(jnp.bfloat16).reshape(PASSAGES, PLEN, XW)
    passage_ids = (owners * PASS_DEV + slots).astype(jnp.int32)
    score_scale = HD ** (-0.5)

    def one_group(group):
        query_part, gate_part, cot_part, id_part = group
        flat_ids = id_part.reshape(-1).astype(jnp.int32)
        group_keys = key_table[flat_ids].reshape(BLK_DEV, NPB * PLEN, HEADS, HD).astype(jnp.float32)
        group_values = value_table[flat_ids].reshape(BLK_DEV, NPB * PLEN, HEADS, HD).astype(jnp.float32)
        query_wide = query_part.astype(jnp.float32)
        scores = jnp.einsum('bqhd,bkhd->bhqk', query_wide, group_keys) * score_scale
        shifted = scores - lax.optimization_barrier(jnp.max(scores, axis=-1, keepdims=True))
        weights = jnp.exp(shifted)
        weights = weights / lax.optimization_barrier(jnp.sum(weights, axis=-1, keepdims=True))
        weights_half = lax.optimization_barrier(weights.astype(jnp.bfloat16)).astype(jnp.float32)
        grad_in = jax.nn.sigmoid(gate_part.astype(jnp.float32)) * cot_part.astype(jnp.float32)
        grad_in = lax.optimization_barrier(grad_in.astype(jnp.bfloat16)).astype(jnp.float32)
        attended = jnp.einsum('bhqk,bkhd->bqhd', weights_half, group_values)
        row_delta = lax.optimization_barrier(jnp.sum(grad_in * attended, axis=-1))
        grad_weights = jnp.einsum('bqhd,bkhd->bhqk', grad_in, group_values)
        grad_scores = weights * (grad_weights - jnp.transpose(row_delta, (0, 2, 1))[..., None])
        grad_half = lax.optimization_barrier(grad_scores.astype(jnp.bfloat16)).astype(jnp.float32)
        grad_query = jnp.einsum('bhqk,bkhd->bqhd', grad_half, group_keys) * score_scale
        grad_key = jnp.einsum('bhqk,bqhd->bkhd', grad_half, query_wide) * score_scale
        grad_value = jnp.einsum('bhqk,bqhd->bkhd', weights_half, grad_in)
        return (grad_query.reshape(BLK_DEV * BLK, XW), grad_key.reshape(BLK_DEV * NPB, PLEN, XW), grad_value.reshape(BLK_DEV * NPB, PLEN, XW))
    groups = (queries.reshape(N_ST, BLK_DEV, BLK, HEADS, HD), gate_pre.reshape(N_ST, BLK_DEV, BLK, HEADS, HD), cotangent.reshape(N_ST, BLK_DEV, BLK, HEADS, HD), passage_ids.reshape(N_ST, BLK_DEV, NPB))
    grad_queries, slot_keys, slot_values = lax.map(one_group, groups)
    grad_queries = grad_queries.reshape(TOKENS, XW)
    every_id = passage_ids.reshape(-1)
    passage_keys = jnp.zeros((PASSAGES, PLEN, XW), jnp.float32).at[every_id].add(slot_keys.reshape(BLOCKS * NPB, PLEN, XW))
    passage_values = jnp.zeros((PASSAGES, PLEN, XW), jnp.float32).at[every_id].add(slot_values.reshape(BLOCKS * NPB, PLEN, XW))
    passage_keys = passage_keys.astype(jnp.bfloat16).reshape(ROWS, XW)
    passage_values = passage_values.astype(jnp.bfloat16).reshape(ROWS, XW)
    grad_normed = jnp.dot(passage_keys, w_key.T, preferred_element_type=jnp.float32) + jnp.dot(passage_values, w_value.T, preferred_element_type=jnp.float32)
    grad_w_value = jnp.dot(normed.T, passage_values, preferred_element_type=jnp.float32)
    unit_rows = store_rows * row_inverse
    grad_unit = grad_normed * store_gain
    grad_store = row_inverse * (grad_unit - unit_rows * lax.optimization_barrier(jnp.mean(grad_unit * unit_rows, axis=-1, keepdims=True)))
    return (grad_queries, grad_store, grad_w_value)
```

```python
import functools

import jax
import jax.numpy as jnp
from jax import lax
from jax.experimental import pallas as pl
from jax.experimental.pallas import tpu as pltpu
from jax.sharding import PartitionSpec as P

HD = 128
PLEN = 64


EPS = 1e-06


def row_scale(store_rows):
    return lax.rsqrt(jnp.mean(store_rows * store_rows, axis=-1, keepdims=True) + EPS)


def contract(left, right):
    return lax.dot_general(
        left, right, (((1,), (1,)), ((), ())), preferred_element_type=jnp.float32
    )


def passage_plan(queries, gate_pre, cotangent, store, store_gain, w_key, w_value, owners, slots):
    st_size = lax.axis_size("st")
    tp_size = lax.axis_size("tp")
    blocks, per_block = owners.shape
    tok_rows, local_width = queries.shape
    head_dim = HD
    local_heads = local_width // head_dim
    block_len = tok_rows // blocks
    passage_len = PLEN
    rows_dev = store.shape[0]
    passages = rows_dev // passage_len
    slot_count = blocks * per_block
    slot_cap = (2 * slot_count + st_size - 1) // st_size
    store_rows = store.astype(jnp.float32)
    row_inverse = row_scale(store_rows)
    normed = (store_rows * row_inverse * store_gain).astype(jnp.bfloat16)
    key_table = jnp.dot(normed, w_key, preferred_element_type=jnp.float32).astype(jnp.bfloat16)
    value_table = jnp.dot(normed, w_value, preferred_element_type=jnp.float32).astype(jnp.bfloat16)
    key_table = key_table.reshape(passages, passage_len, local_width)
    value_table = value_table.reshape(passages, passage_len, local_width)
    owner_flat = owners.reshape(slot_count)
    slot_flat = slots.reshape(slot_count)
    slot_order = jnp.arange(slot_count, dtype=jnp.int32)
    earlier_same = (owner_flat[:, None] == owner_flat[None, :]) & (
        slot_order[None, :] < slot_order[:, None]
    )
    slot_rank = jnp.sum(earlier_same.astype(jnp.int32), axis=1)
    position = owner_flat * slot_cap + slot_rank
    places = jnp.arange(st_size * slot_cap, dtype=jnp.int32)
    slot_hits = position[:, None] == places[None, :]
    requests = jnp.sum(jnp.where(slot_hits, slot_flat[:, None], 0), axis=0)
    requests = requests.reshape(st_size, slot_cap)
    asked_ids = lax.all_to_all(requests, "st", split_axis=0, concat_axis=0, tiled=True)
    asked_flat = asked_ids.reshape(-1)
    shape_out = asked_ids.shape + (passage_len, local_width)
    picked_keys = jnp.take(key_table, asked_flat, axis=0).reshape(shape_out)
    picked_values = jnp.take(value_table, asked_flat, axis=0).reshape(shape_out)
    sent_keys = lax.all_to_all(picked_keys, "st", split_axis=0, concat_axis=0, tiled=True)
    sent_values = lax.all_to_all(picked_values, "st", split_axis=0, concat_axis=0, tiled=True)
    got_keys, got_values, asked_ids = (sent_keys, sent_values, asked_ids)
    span = per_block * passage_len
    mine_keys = jnp.take(
        got_keys.reshape(st_size * slot_cap, passage_len, local_width), position, axis=0
    )
    mine_values = jnp.take(
        got_values.reshape(st_size * slot_cap, passage_len, local_width), position, axis=0
    )
    mine_keys = mine_keys.reshape(blocks, span, local_heads, head_dim)
    mine_values = mine_values.reshape(blocks, span, local_heads, head_dim)
    score_scale = head_dim ** (-0.5)
    query_blocks = queries.reshape(blocks, block_len, local_heads, head_dim)
    gate_open = jax.nn.sigmoid(gate_pre.astype(jnp.float32))
    grad_in = (gate_open * cotangent.astype(jnp.float32)).astype(jnp.bfloat16)
    grad_in = grad_in.reshape(blocks, block_len, local_heads, head_dim)
    scores = (
        jnp.einsum("bqhd,bkhd->bhqk", query_blocks, mine_keys, preferred_element_type=jnp.float32)
        * score_scale
    )
    shifted = scores - jnp.max(scores, axis=-1, keepdims=True)
    weights = jnp.exp(shifted)
    weights = weights / jnp.sum(weights, axis=-1, keepdims=True)
    weights_half = weights.astype(jnp.bfloat16)
    attended = jnp.einsum(
        "bhqk,bkhd->bqhd", weights_half, mine_values, preferred_element_type=jnp.float32
    )
    row_delta = jnp.sum(grad_in.astype(jnp.float32) * attended, axis=-1)
    grad_weights = jnp.einsum(
        "bqhd,bkhd->bhqk", grad_in, mine_values, preferred_element_type=jnp.float32
    )
    grad_scores = weights * (grad_weights - jnp.transpose(row_delta, (0, 2, 1))[..., None])
    grad_half = grad_scores.astype(jnp.bfloat16)
    grad_queries = (
        jnp.einsum("bhqk,bkhd->bqhd", grad_half, mine_keys, preferred_element_type=jnp.float32)
        * score_scale
    )
    grad_queries = grad_queries.reshape(tok_rows, local_width)
    grad_keys = (
        jnp.einsum("bhqk,bqhd->bkhd", grad_half, query_blocks, preferred_element_type=jnp.float32)
        * score_scale
    )
    grad_values = jnp.einsum(
        "bhqk,bqhd->bkhd", weights_half, grad_in, preferred_element_type=jnp.float32
    )
    grad_keys = grad_keys.reshape(slot_count, passage_len, local_width)
    grad_values = grad_values.reshape(slot_count, passage_len, local_width)
    empty_slots = jnp.zeros((st_size * slot_cap, passage_len, local_width), jnp.bfloat16)
    outgoing_keys = empty_slots.at[position].set(grad_keys.astype(jnp.bfloat16))
    outgoing_values = empty_slots.at[position].set(grad_values.astype(jnp.bfloat16))
    back_keys, back_values = (
        lax.all_to_all(outgoing_keys, "st", split_axis=0, concat_axis=0, tiled=True),
        lax.all_to_all(outgoing_values, "st", split_axis=0, concat_axis=0, tiled=True),
    )
    asked_flat = asked_ids.reshape(-1)
    owner_pick = (asked_flat[None, :] == jnp.arange(passages, dtype=jnp.int32)[:, None]).astype(
        jnp.bfloat16
    )
    passage_keys = jnp.dot(
        owner_pick,
        back_keys.reshape(st_size * slot_cap, passage_len * local_width),
        preferred_element_type=jnp.float32,
    )
    passage_values = jnp.dot(
        owner_pick,
        back_values.reshape(st_size * slot_cap, passage_len * local_width),
        preferred_element_type=jnp.float32,
    )
    passage_keys = passage_keys.astype(jnp.bfloat16).reshape(rows_dev, local_width)
    passage_values = passage_values.astype(jnp.bfloat16).reshape(rows_dev, local_width)
    weight_terms = lax.dot_general(
        normed, passage_values, (((0,), (0,)), ((), ())), preferred_element_type=jnp.float32
    )
    grad_w_value = lax.psum_scatter(weight_terms, "st", scatter_dimension=0, tiled=True)
    quarter = rows_dev // tp_size
    whole_key, whole_value = (
        lax.all_gather(w_key, "tp", axis=1, tiled=True),
        lax.all_gather(w_value, "tp", axis=1, tiled=True),
    )
    own_keys, own_values = (
        lax.all_to_all(passage_keys, "tp", split_axis=0, concat_axis=1, tiled=True),
        lax.all_to_all(passage_values, "tp", split_axis=0, concat_axis=1, tiled=True),
    )
    grad_normed = contract(own_keys, whole_key) + contract(own_values, whole_value)
    first_row = lax.axis_index("tp") * quarter
    own_rows = lax.dynamic_slice_in_dim(store_rows, first_row, quarter, 0)
    own_inverse = lax.dynamic_slice_in_dim(row_inverse, first_row, quarter, 0)
    unit_rows = own_rows * own_inverse
    grad_unit = grad_normed * store_gain
    grad_store = own_inverse * (
        grad_unit - unit_rows * jnp.mean(grad_unit * unit_rows, axis=-1, keepdims=True)
    )
    return (grad_queries, grad_store, grad_w_value)


FAR = -1e30
MESH = pl.DeviceIdType.MESH


def place_of(index, n):
    odd = index % 2
    return (1 - odd) * (index // 2) + odd * (n - 1 - index // 2)


def index_at(place, n):
    place = (place + 2 * n) % n
    back = place // (n // 2)
    return (1 - back) * (2 * place) + back * (2 * (n - 1 - place) + 1)


def greet(right, left):
    barrier = pltpu.get_barrier_semaphore()
    for neighbour in (left, right):
        pl.semaphore_signal(barrier, inc=1, device_id={"st": neighbour}, device_id_type=MESH)
    pl.semaphore_wait(barrier, 2)


def gather_kernel(n, q_ref, g_ref, q_all, g_all, send_sem, recv_sem, own_sem):
    me = lax.axis_index("st")
    place = place_of(me, n)
    right, left = index_at(place + 1, n), index_at(place - 1, n)
    half_rows = q_ref.shape[0] // 2
    greet(right, left)
    own = []
    for number, (src, dst) in enumerate(((q_ref, q_all), (g_ref, g_all))):
        copy = pltpu.make_async_copy(src, dst.at[me], own_sem.at[number])
        copy.start()
        own.append(copy)
    hops = n // 2

    def piece(side, step, part):
        number, half = part // 2, part % 2
        src, dst = ((q_ref, q_all), (g_ref, g_all))[number]
        origin = index_at(place - step, n) if side == 0 else index_at(place + step, n)
        rows = pl.ds(half * half_rows, half_rows)
        return pltpu.make_async_remote_copy(
            src_ref=src.at[rows] if step == 0 else dst.at[origin, rows],
            dst_ref=dst.at[origin, rows],
            send_sem=send_sem.at[side, step, part],
            recv_sem=recv_sem.at[side, step, part],
            device_id={"st": right if side == 0 else left},
            device_id_type=MESH,
        )

    started = []
    for step in range(hops):
        for part in range(4):
            for side in range(2):
                if step > 0 and (step < hops - 1 or part % 2 == side):
                    piece(side, step - 1, part).wait_recv()
                if step < hops - 1 or part % 2 == side:
                    copy = piece(side, step, part)
                    copy.start()
                    started.append(copy)
    for part in range(4):
        for side in range(2):
            if part % 2 != side:
                piece(side, hops - 2, part).wait_recv()
    for part in range(4):
        piece(part % 2, hops - 1, part).wait_recv()
    for copy in own:
        copy.wait()
    for copy in started:
        copy.wait_send()


def ring_gather(queries, grad_in, n):
    rows, width = queries.shape
    hops = n // 2
    shape = jax.ShapeDtypeStruct((n, rows, width), jnp.bfloat16)
    vmem = pl.BlockSpec(memory_space=pltpu.VMEM)
    return pl.pallas_call(
        functools.partial(gather_kernel, n),
        out_shape=(shape, shape),
        in_specs=[vmem, vmem],
        out_specs=(vmem, vmem),
        scratch_shapes=[
            pltpu.SemaphoreType.DMA((2, hops, 4)),
            pltpu.SemaphoreType.DMA((2, hops, 4)),
            pltpu.SemaphoreType.DMA((2,)),
        ],
        compiler_params=pltpu.CompilerParams(collective_id=0, has_side_effects=True, vmem_limit_bytes=40 << 20),
        name="ring_gather",
    )(queries, grad_in)


def scatter_kernel(n, parts, x_ref, out_ref, send_buf, recv_buf, send_sem, recv_sem):
    me = lax.axis_index("st")
    place = place_of(me, n)
    right, left = index_at(place + 1, n), index_at(place - 1, n)
    rows = x_ref.shape[1]
    span = rows // parts
    greet(right, left)
    hops = n // 2

    def used(side, step, part):
        return step > 0 or (part < parts // 2) == (side == 0)

    def piece(side, step, part):
        return pltpu.make_async_remote_copy(
            src_ref=send_buf.at[side, step, pl.ds(part * span, span)],
            dst_ref=recv_buf.at[side, step, pl.ds(part * span, span)],
            send_sem=send_sem.at[side, step, part],
            recv_sem=recv_sem.at[side, step, part],
            device_id={"st": right if side == 0 else left},
            device_id_type=MESH,
        )

    started = []
    for step in range(hops):
        for part in range(parts):
            for side in range(2):
                if not used(side, step, part):
                    continue
                distance = hops - step
                dest = index_at(place + distance, n) if side == 0 else index_at(place - distance, n)
                at = pl.ds(part * span, span)
                total = x_ref[dest, at]
                if step > 0 and used(side, step - 1, part):
                    piece(side, step - 1, part).wait_recv()
                    total = (total.astype(jnp.float32) + recv_buf[side, step - 1, at].astype(jnp.float32)).astype(jnp.bfloat16)
                send_buf[side, step, at] = total
                copy = piece(side, step, part)
                copy.start()
                started.append(copy)
    for part in range(parts):
        at = pl.ds(part * span, span)
        total = x_ref[me, at].astype(jnp.float32)
        for side in range(2):
            piece(side, hops - 1, part).wait_recv()
            total = total + recv_buf[side, hops - 1, at].astype(jnp.float32)
        out_ref[at] = total
    for copy in started:
        copy.wait_send()


def ring_scatter(terms, n):
    rows, width = terms.shape[1:]
    hops = n // 2
    parts = 4
    vmem = pl.BlockSpec(memory_space=pltpu.VMEM)
    return pl.pallas_call(
        functools.partial(scatter_kernel, n, parts),
        out_shape=jax.ShapeDtypeStruct((rows, width), jnp.float32),
        in_specs=[vmem],
        out_specs=vmem,
        scratch_shapes=[
            pltpu.VMEM((2, hops, rows, width), jnp.bfloat16),
            pltpu.VMEM((2, hops, rows, width), jnp.bfloat16),
            pltpu.SemaphoreType.DMA((2, hops, parts)),
            pltpu.SemaphoreType.DMA((2, hops, parts)),
        ],
        compiler_params=pltpu.CompilerParams(collective_id=1, has_side_effects=True, vmem_limit_bytes=40 << 20),
        name="ring_scatter",
    )(terms)


NT = (((1,), (1,)), ((), ()))
TN = (((0,), (0,)), ((), ()))


def dot(left, right, dims=(((1,), (0,)), ((), ()))):
    return lax.dot_general(left, right, dims, preferred_element_type=jnp.float32)


def stats_kernel(blocks, heads, ids, q_ref, g_ref, k_ref, v_ref, out_ref):
    scale = HD ** (-0.5)
    block_len = q_ref.shape[1] // blocks

    @pl.loop(0, blocks)
    def _(block):
        picked = ids[pl.program_id(0) * blocks + block]

        @pl.when(picked < 0)
        def _():
            for head in range(heads):
                out_ref[block, 2 * head] = jnp.full((block_len,), FAR, jnp.float32)
                out_ref[block, 2 * head + 1] = jnp.zeros((block_len,), jnp.float32)

        @pl.when(picked >= 0)
        def _():
            tokens = pl.ds(pl.multiple_of(block * block_len, block_len), block_len)
            for head in range(heads):
                cols = pl.ds(head * HD, HD)
                scores = dot(k_ref[picked, :, cols], q_ref[0, tokens, cols], NT) * scale
                grads = dot(v_ref[picked, :, cols], g_ref[0, tokens, cols], NT)
                top = jnp.max(scores, axis=0, keepdims=True)
                raised = jnp.exp(scores - top)
                total = jnp.sum(raised, axis=0, keepdims=True)
                mean = jnp.sum(raised * grads, axis=0, keepdims=True) / total
                out_ref[block, pl.ds(2 * head, 1)] = top + jnp.log(total)
                out_ref[block, pl.ds(2 * head + 1, 1)] = mean


def grads_kernel(blocks, heads, ids, q_ref, g_ref, k_ref, v_ref, s_ref, dq_ref, pk_ref, pv_ref, dk_acc, dv_acc):
    scale = HD ** (-0.5)
    block_len = q_ref.shape[1] // blocks

    @pl.when(pl.program_id(0) == 0)
    def _():
        dk_acc[...] = jnp.zeros_like(dk_acc)
        dv_acc[...] = jnp.zeros_like(dv_acc)

    @pl.loop(0, blocks)
    def _(block):
        picked = ids[pl.program_id(0) * blocks + block]
        tokens = pl.ds(pl.multiple_of(block * block_len, block_len), block_len)

        @pl.when(picked < 0)
        def _():
            dq_ref[0, tokens] = jnp.zeros((block_len, heads * HD), jnp.bfloat16)

        @pl.when(picked >= 0)
        def _():
            for head in range(heads):
                cols = pl.ds(head * HD, HD)
                keys = k_ref[picked, :, cols]
                tok_q, tok_g = q_ref[0, tokens, cols], g_ref[0, tokens, cols]
                scores = dot(keys, tok_q, NT) * scale
                grads = dot(v_ref[picked, :, cols], tok_g, NT)
                weights = jnp.exp(scores - s_ref[block, pl.ds(2 * head, 1)])
                half = (weights * (grads - s_ref[block, pl.ds(2 * head + 1, 1)])).astype(jnp.bfloat16)
                dq_ref[0, tokens, cols] = (dot(half, keys, TN) * scale).astype(jnp.bfloat16)
                dk_acc[picked, :, cols] += dot(half, tok_q) * scale
                dv_acc[picked, :, cols] += dot(weights.astype(jnp.bfloat16), tok_g)

    @pl.when(pl.program_id(0) == pl.num_programs(0) - 1)
    def _():
        pk_ref[...] = dk_acc[...].astype(jnp.bfloat16)
        pv_ref[...] = dv_acc[...].astype(jnp.bfloat16)


def query_plan(queries, gate_pre, cotangent, store, store_gain, w_key, w_value, owners, slots):
    n = lax.axis_size("st")
    tp_size = lax.axis_size("tp")
    me = lax.axis_index("st")
    blocks, per_block = owners.shape
    tok_rows, local_width = queries.shape
    heads = local_width // HD
    block_len = tok_rows // blocks
    rows_dev = store.shape[0]
    passages = rows_dev // PLEN
    named = owners * passages + slots
    all_named = lax.all_gather(named, "st", axis=0, tiled=True)
    held = all_named - me * passages
    ids = jnp.max(jnp.where((held >= 0) & (held < passages), held, -1), axis=1)
    gate_open = jax.nn.sigmoid(gate_pre.astype(jnp.float32))
    grad_in = (gate_open * cotangent.astype(jnp.float32)).astype(jnp.bfloat16)
    q_all, g_all = ring_gather(queries, grad_in, n)
    store_rows = store.astype(jnp.float32)
    row_inverse = row_scale(store_rows)
    normed = (store_rows * row_inverse * store_gain).astype(jnp.bfloat16)
    key_table = jnp.dot(normed, w_key, preferred_element_type=jnp.float32).astype(jnp.bfloat16)
    value_table = jnp.dot(normed, w_value, preferred_element_type=jnp.float32).astype(jnp.bfloat16)
    key_table = key_table.reshape(passages, PLEN, local_width)
    value_table = value_table.reshape(passages, PLEN, local_width)
    token_spec = pl.BlockSpec((1, tok_rows, local_width), lambda i, ids: (i, 0, 0))
    table_spec = pl.BlockSpec((passages, PLEN, local_width), lambda i, ids: (0, 0, 0))
    stat_spec = pl.BlockSpec((blocks, 2 * heads, block_len), lambda i, ids: (i, 0, 0))
    stats = pl.pallas_call(
        functools.partial(stats_kernel, blocks, heads),
        out_shape=jax.ShapeDtypeStruct((n * blocks, 2 * heads, block_len), jnp.float32),
        grid_spec=pltpu.PrefetchScalarGridSpec(
            num_scalar_prefetch=1,
            grid=(n,),
            in_specs=[token_spec, token_spec, table_spec, table_spec],
            out_specs=stat_spec,
        ),
        name="stats",
    )(ids, q_all, g_all, key_table, value_table)
    every = lax.all_gather(stats, "st", axis=0)
    every = every.reshape(n, n * blocks, heads, 2, block_len)
    logs, means = every[:, :, :, 0], every[:, :, :, 1]
    top = jnp.max(logs, axis=0)
    shares = jnp.exp(logs - top)
    total = jnp.sum(shares, axis=0)
    log_all = top + jnp.log(total)
    delta = jnp.sum(shares * means, axis=0) / total
    joined = jnp.stack([log_all, delta], axis=2).reshape(n * blocks, 2 * heads, block_len)
    dq, passage_keys, passage_values = pl.pallas_call(
        functools.partial(grads_kernel, blocks, heads),
        out_shape=(
            jax.ShapeDtypeStruct((n, tok_rows, local_width), jnp.bfloat16),
            jax.ShapeDtypeStruct((passages, PLEN, local_width), jnp.bfloat16),
            jax.ShapeDtypeStruct((passages, PLEN, local_width), jnp.bfloat16),
        ),
        grid_spec=pltpu.PrefetchScalarGridSpec(
            num_scalar_prefetch=1,
            grid=(n,),
            in_specs=[token_spec, token_spec, table_spec, table_spec, stat_spec],
            out_specs=(token_spec, table_spec, table_spec),
            scratch_shapes=[pltpu.VMEM((passages, PLEN, local_width), jnp.float32)] * 2,
        ),
        name="grads",
    )(ids, q_all, g_all, key_table, value_table, joined)
    passage_keys = passage_keys.reshape(rows_dev, local_width)
    passage_values = passage_values.reshape(rows_dev, local_width)
    weight_terms = lax.dot_general(
        normed, passage_values, (((0,), (0,)), ((), ())), preferred_element_type=jnp.float32
    )
    grad_w_value = lax.psum_scatter(weight_terms, "st", scatter_dimension=0, tiled=True)
    grad_queries = ring_scatter(dq, n)
    quarter = rows_dev // tp_size
    whole_key, whole_value = (
        lax.all_gather(w_key, "tp", axis=1, tiled=True),
        lax.all_gather(w_value, "tp", axis=1, tiled=True),
    )
    own_keys, own_values = (
        lax.all_to_all(passage_keys, "tp", split_axis=0, concat_axis=1, tiled=True),
        lax.all_to_all(passage_values, "tp", split_axis=0, concat_axis=1, tiled=True),
    )
    grad_normed = contract(own_keys, whole_key) + contract(own_values, whole_value)
    first_row = lax.axis_index("tp") * quarter
    own_rows = lax.dynamic_slice_in_dim(store, first_row, quarter, 0).astype(jnp.float32)
    own_inverse = row_scale(own_rows)
    unit_rows = own_rows * own_inverse
    grad_unit = grad_normed * store_gain
    grad_store = own_inverse * (
        grad_unit - unit_rows * jnp.mean(grad_unit * unit_rows, axis=-1, keepdims=True)
    )
    return (grad_queries, grad_store, grad_w_value)


def local(*arrays):
    queries, owners = arrays[0], arrays[7]
    n = lax.axis_size("st")
    slot_cap = (2 * owners.size + n - 1) // n
    if n % 2 == 0 and n >= 4 and 8 * slot_cap * PLEN >= 3 * queries.shape[0]:
        return query_plan(*arrays)
    return passage_plan(*arrays)


def solution(mesh):
    placed = (
        P("st", "tp"),
        P("st", "tp"),
        P("st", "tp"),
        P("st", None),
        P(),
        P(None, "tp"),
        P(None, "tp"),
        P("st", None),
        P("st", None),
    )
    return jax.shard_map(
        local,
        mesh=mesh,
        in_specs=placed,
        out_specs=(P("st", "tp"), P(("st", "tp"), None), P("st", "tp")),
        check_vma=False,
    )
```

```python
import functools

import jax
import jax.numpy as jnp
from jax import lax
from jax.experimental import pallas as pl
from jax.experimental.pallas import tpu as pltpu
from jax.sharding import PartitionSpec as P

HD = 128
PLEN = 64


EPS = 1e-06


def row_scale(store_rows):
    return lax.rsqrt(jnp.mean(store_rows * store_rows, axis=-1, keepdims=True) + EPS)


def contract(left, right):
    return lax.dot_general(
        left, right, (((1,), (1,)), ((), ())), preferred_element_type=jnp.float32
    )


def passage_plan(queries, gate_pre, cotangent, store, store_gain, w_key, w_value, owners, slots):
    st_size = lax.axis_size("st")
    tp_size = lax.axis_size("tp")
    blocks, per_block = owners.shape
    tok_rows, local_width = queries.shape
    head_dim = HD
    local_heads = local_width // head_dim
    block_len = tok_rows // blocks
    passage_len = PLEN
    rows_dev = store.shape[0]
    passages = rows_dev // passage_len
    slot_count = blocks * per_block
    slot_cap = (2 * slot_count + st_size - 1) // st_size
    store_rows = store.astype(jnp.float32)
    row_inverse = row_scale(store_rows)
    normed = (store_rows * row_inverse * store_gain).astype(jnp.bfloat16)
    key_table = jnp.dot(normed, w_key, preferred_element_type=jnp.float32).astype(jnp.bfloat16)
    value_table = jnp.dot(normed, w_value, preferred_element_type=jnp.float32).astype(jnp.bfloat16)
    key_table = key_table.reshape(passages, passage_len, local_width)
    value_table = value_table.reshape(passages, passage_len, local_width)
    owner_flat = owners.reshape(slot_count)
    slot_flat = slots.reshape(slot_count)
    slot_order = jnp.arange(slot_count, dtype=jnp.int32)
    earlier_same = (owner_flat[:, None] == owner_flat[None, :]) & (
        slot_order[None, :] < slot_order[:, None]
    )
    slot_rank = jnp.sum(earlier_same.astype(jnp.int32), axis=1)
    position = owner_flat * slot_cap + slot_rank
    places = jnp.arange(st_size * slot_cap, dtype=jnp.int32)
    slot_hits = position[:, None] == places[None, :]
    requests = jnp.sum(jnp.where(slot_hits, slot_flat[:, None], 0), axis=0)
    requests = requests.reshape(st_size, slot_cap)
    asked_ids = lax.all_to_all(requests, "st", split_axis=0, concat_axis=0, tiled=True)
    asked_flat = asked_ids.reshape(-1)
    shape_out = asked_ids.shape + (passage_len, local_width)
    picked_keys = jnp.take(key_table, asked_flat, axis=0).reshape(shape_out)
    picked_values = jnp.take(value_table, asked_flat, axis=0).reshape(shape_out)
    sent_keys = lax.all_to_all(picked_keys, "st", split_axis=0, concat_axis=0, tiled=True)
    sent_values = lax.all_to_all(picked_values, "st", split_axis=0, concat_axis=0, tiled=True)
    got_keys, got_values, asked_ids = (sent_keys, sent_values, asked_ids)
    span = per_block * passage_len
    mine_keys = jnp.take(
        got_keys.reshape(st_size * slot_cap, passage_len, local_width), position, axis=0
    )
    mine_values = jnp.take(
        got_values.reshape(st_size * slot_cap, passage_len, local_width), position, axis=0
    )
    mine_keys = mine_keys.reshape(blocks, span, local_heads, head_dim)
    mine_values = mine_values.reshape(blocks, span, local_heads, head_dim)
    score_scale = head_dim ** (-0.5)
    query_blocks = queries.reshape(blocks, block_len, local_heads, head_dim)
    gate_open = jax.nn.sigmoid(gate_pre.astype(jnp.float32))
    grad_in = (gate_open * cotangent.astype(jnp.float32)).astype(jnp.bfloat16)
    grad_in = grad_in.reshape(blocks, block_len, local_heads, head_dim)
    scores = (
        jnp.einsum("bqhd,bkhd->bhqk", query_blocks, mine_keys, preferred_element_type=jnp.float32)
        * score_scale
    )
    shifted = scores - jnp.max(scores, axis=-1, keepdims=True)
    weights = jnp.exp(shifted)
    weights = weights / jnp.sum(weights, axis=-1, keepdims=True)
    weights_half = weights.astype(jnp.bfloat16)
    attended = jnp.einsum(
        "bhqk,bkhd->bqhd", weights_half, mine_values, preferred_element_type=jnp.float32
    )
    row_delta = jnp.sum(grad_in.astype(jnp.float32) * attended, axis=-1)
    grad_weights = jnp.einsum(
        "bqhd,bkhd->bhqk", grad_in, mine_values, preferred_element_type=jnp.float32
    )
    grad_scores = weights * (grad_weights - jnp.transpose(row_delta, (0, 2, 1))[..., None])
    grad_half = grad_scores.astype(jnp.bfloat16)
    grad_queries = (
        jnp.einsum("bhqk,bkhd->bqhd", grad_half, mine_keys, preferred_element_type=jnp.float32)
        * score_scale
    )
    grad_queries = grad_queries.reshape(tok_rows, local_width)
    grad_keys = (
        jnp.einsum("bhqk,bqhd->bkhd", grad_half, query_blocks, preferred_element_type=jnp.float32)
        * score_scale
    )
    grad_values = jnp.einsum(
        "bhqk,bqhd->bkhd", weights_half, grad_in, preferred_element_type=jnp.float32
    )
    grad_keys = grad_keys.reshape(slot_count, passage_len, local_width)
    grad_values = grad_values.reshape(slot_count, passage_len, local_width)
    empty_slots = jnp.zeros((st_size * slot_cap, passage_len, local_width), jnp.bfloat16)
    outgoing_keys = empty_slots.at[position].set(grad_keys.astype(jnp.bfloat16))
    outgoing_values = empty_slots.at[position].set(grad_values.astype(jnp.bfloat16))
    back_keys, back_values = (
        lax.all_to_all(outgoing_keys, "st", split_axis=0, concat_axis=0, tiled=True),
        lax.all_to_all(outgoing_values, "st", split_axis=0, concat_axis=0, tiled=True),
    )
    asked_flat = asked_ids.reshape(-1)
    owner_pick = (asked_flat[None, :] == jnp.arange(passages, dtype=jnp.int32)[:, None]).astype(
        jnp.bfloat16
    )
    passage_keys = jnp.dot(
        owner_pick,
        back_keys.reshape(st_size * slot_cap, passage_len * local_width),
        preferred_element_type=jnp.float32,
    )
    passage_values = jnp.dot(
        owner_pick,
        back_values.reshape(st_size * slot_cap, passage_len * local_width),
        preferred_element_type=jnp.float32,
    )
    passage_keys = passage_keys.astype(jnp.bfloat16).reshape(rows_dev, local_width)
    passage_values = passage_values.astype(jnp.bfloat16).reshape(rows_dev, local_width)
    weight_terms = lax.dot_general(
        normed, passage_values, (((0,), (0,)), ((), ())), preferred_element_type=jnp.float32
    )
    grad_w_value = lax.psum_scatter(weight_terms, "st", scatter_dimension=0, tiled=True)
    quarter = rows_dev // tp_size
    whole_key, whole_value = (
        lax.all_gather(w_key, "tp", axis=1, tiled=True),
        lax.all_gather(w_value, "tp", axis=1, tiled=True),
    )
    own_keys, own_values = (
        lax.all_to_all(passage_keys, "tp", split_axis=0, concat_axis=1, tiled=True),
        lax.all_to_all(passage_values, "tp", split_axis=0, concat_axis=1, tiled=True),
    )
    grad_normed = contract(own_keys, whole_key) + contract(own_values, whole_value)
    first_row = lax.axis_index("tp") * quarter
    own_rows = lax.dynamic_slice_in_dim(store_rows, first_row, quarter, 0)
    own_inverse = lax.dynamic_slice_in_dim(row_inverse, first_row, quarter, 0)
    unit_rows = own_rows * own_inverse
    grad_unit = grad_normed * store_gain
    grad_store = own_inverse * (
        grad_unit - unit_rows * jnp.mean(grad_unit * unit_rows, axis=-1, keepdims=True)
    )
    return (grad_queries, grad_store, grad_w_value)


FAR = -1e30
MESH = pl.DeviceIdType.MESH


def place_of(index, n):
    odd = index % 2
    return (1 - odd) * (index // 2) + odd * (n - 1 - index // 2)


def index_at(place, n):
    place = (place + 2 * n) % n
    back = place // (n // 2)
    return (1 - back) * (2 * place) + back * (2 * (n - 1 - place) + 1)


def greet(others):
    barrier = pltpu.get_barrier_semaphore()
    for axis, other in others:
        pl.semaphore_signal(barrier, inc=1, device_id={axis: other}, device_id_type=MESH)
    pl.semaphore_wait(barrier, len(others))


def gather_kernel(n, q_ref, g_ref, i_ref, q_all, g_all, i_all, send_sem, recv_sem, own_sem):
    me = lax.axis_index("st")
    place = place_of(me, n)
    right, left = index_at(place + 1, n), index_at(place - 1, n)
    half_rows = q_ref.shape[0] // 2
    pairs = ((q_ref, q_all), (g_ref, g_all), (i_ref, i_all))
    greet((("st", left), ("st", right)))
    own = []
    for number, (src, dst) in enumerate(pairs):
        copy = pltpu.make_async_copy(src, dst.at[me], own_sem.at[number])
        copy.start()
        own.append(copy)
    hops = n // 2
    parts = ((2, 0), (0, 0), (0, 1), (1, 0), (1, 1))

    def last_on(side, part):
        return parts[part][1] == side

    def piece(side, step, part):
        number, half = parts[part]
        src, dst = pairs[number]
        origin = index_at(place - step, n) if side == 0 else index_at(place + step, n)
        rows = pl.ds(0, i_ref.shape[0]) if number == 2 else pl.ds(half * half_rows, half_rows)
        return pltpu.make_async_remote_copy(
            src_ref=src.at[rows] if step == 0 else dst.at[origin, rows],
            dst_ref=dst.at[origin, rows],
            send_sem=send_sem.at[side, step, part],
            recv_sem=recv_sem.at[side, step, part],
            device_id={"st": right if side == 0 else left},
            device_id_type=MESH,
        )

    started = []
    for step in range(hops):
        for part in range(5):
            for side in range(2):
                if step < hops - 1 or last_on(side, part):
                    if step > 0:
                        piece(side, step - 1, part).wait_recv()
                    copy = piece(side, step, part)
                    copy.start()
                    started.append(copy)
    for part in range(5):
        for side in range(2):
            if not last_on(side, part):
                piece(side, hops - 2, part).wait_recv()
    for part in range(5):
        piece(parts[part][1], hops - 1, part).wait_recv()
    for copy in own:
        copy.wait()
    for copy in started:
        copy.wait_send()


def ring_gather(queries, grad_in, named, n):
    hops = n // 2
    vmem = pl.BlockSpec(memory_space=pltpu.VMEM)
    sources = (queries, grad_in, named)
    return pl.pallas_call(
        functools.partial(gather_kernel, n),
        out_shape=tuple(jax.ShapeDtypeStruct((n,) + x.shape, x.dtype) for x in sources),
        in_specs=[vmem] * 3,
        out_specs=(vmem,) * 3,
        scratch_shapes=[
            pltpu.SemaphoreType.DMA((2, hops, 5)),
            pltpu.SemaphoreType.DMA((2, hops, 5)),
            pltpu.SemaphoreType.DMA((3,)),
        ],
        cost_estimate=pl.CostEstimate(flops=10**10, bytes_accessed=10**7, transcendentals=0),
        compiler_params=pltpu.CompilerParams(collective_id=0, has_side_effects=True, vmem_limit_bytes=40 << 20),
        name="ring_gather",
    )(*sources)


def join_kernel(n, heads, x_ref, out_ref, got, mine, send_sem, recv_sem, own_sem):
    me = lax.axis_index("st")
    peers = [(me + away) % n for away in range(1, n)]
    greet([("st", peer) for peer in peers])

    def piece(phase, away):
        peer = (me + away) % n
        return pltpu.make_async_remote_copy(
            src_ref=x_ref.at[peer] if phase == 0 else mine,
            dst_ref=got.at[me] if phase == 0 else out_ref.at[me],
            send_sem=send_sem.at[phase, away],
            recv_sem=recv_sem.at[phase, away],
            device_id={"st": peer},
            device_id_type=MESH,
        )

    for away in range(1, n):
        piece(0, away).start()
    local = pltpu.make_async_copy(x_ref.at[me], got.at[me], own_sem.at[0])
    local.start()
    local.wait()
    for away in range(1, n):
        piece(0, away).wait()
    for head in range(heads):
        logs = [got[owner, :, 2 * head] for owner in range(n)]
        top = functools.reduce(jnp.maximum, logs)
        shares = [jnp.exp(one - top) for one in logs]
        total = sum(shares)
        mine[:, 2 * head] = top + jnp.log(total)
        mine[:, 2 * head + 1] = sum(share * got[owner, :, 2 * head + 1] for owner, share in enumerate(shares)) / total
    out_ref[me] = mine[...]
    for away in range(1, n):
        piece(1, away).start()
    for away in range(1, n):
        piece(1, away).wait()


def join_stats(stats, n):
    total, rows, width = stats.shape
    blocks = total // n
    vmem = pl.BlockSpec(memory_space=pltpu.VMEM)
    joined = pl.pallas_call(
        functools.partial(join_kernel, n, rows // 2),
        out_shape=jax.ShapeDtypeStruct((n, blocks, rows, width), jnp.float32),
        in_specs=[vmem],
        out_specs=vmem,
        scratch_shapes=[
            pltpu.VMEM((n, blocks, rows, width), jnp.float32),
            pltpu.VMEM((blocks, rows, width), jnp.float32),
            pltpu.SemaphoreType.DMA((2, n)),
            pltpu.SemaphoreType.DMA((2, n)),
            pltpu.SemaphoreType.DMA((1,)),
        ],
        cost_estimate=pl.CostEstimate(flops=10**9, bytes_accessed=10**6, transcendentals=0),
        compiler_params=pltpu.CompilerParams(collective_id=2, has_side_effects=True),
        name="join_stats",
    )(stats.reshape(n, blocks, rows, width))
    return joined.reshape(total, rows, width)


def scatter_kernel(n, tp, parts, x_ref, w_ref, k_ref, v_ref, out_ref, gw_ref, ok_ref, ov_ref, send_buf, recv_buf, send_sem, recv_sem, tp_send, tp_recv, own_sem):
    me = lax.axis_index("st")
    mine = lax.axis_index("tp")
    place = place_of(me, n)
    right, left = index_at(place + 1, n), index_at(place - 1, n)
    tokens = x_ref.shape[1]
    greet([("st", left), ("st", right)] + [("tp", (mine + away) % tp) for away in range(1, tp)])
    quarter, width = ok_ref.shape[0], k_ref.shape[1]
    columns = pl.ds(pl.multiple_of(mine * width, 128), width)

    def across(number, away):
        src, dst = ((k_ref, ok_ref), (v_ref, ov_ref))[number]
        peer = (mine + away) % tp
        return pltpu.make_async_remote_copy(
            src_ref=src.at[pl.ds(pl.multiple_of(peer * quarter, 16), quarter)],
            dst_ref=dst.at[:, columns],
            send_sem=tp_send.at[number, away],
            recv_sem=tp_recv.at[number, away],
            device_id={"tp": peer},
            device_id_type=MESH,
        )

    def kept(number):
        src, dst = ((k_ref, ok_ref), (v_ref, ov_ref))[number]
        return pltpu.make_async_copy(
            src.at[pl.ds(pl.multiple_of(mine * quarter, 16), quarter)], dst.at[:, columns], own_sem.at[number]
        )

    for number in range(2):
        kept(number).start()
        for away in range(1, tp):
            across(number, away).start()
    hops = n // 2

    def used(side, step, part):
        return step > 0 or parts[part][3] == side

    def piece(side, step, part):
        number, first, count, _ = parts[part]
        at = pl.ds(number * tokens + first, count)
        return pltpu.make_async_remote_copy(
            src_ref=send_buf.at[side, step, at],
            dst_ref=recv_buf.at[side, step, at],
            send_sem=send_sem.at[side, step, part],
            recv_sem=recv_sem.at[side, step, part],
            device_id={"st": right if side == 0 else left},
            device_id_type=MESH,
        )

    started = []
    for step in range(hops):
        for part, (number, first, count, _) in enumerate(parts):
            for side in range(2):
                if not used(side, step, part):
                    continue
                distance = hops - step
                dest = index_at(place + distance, n) if side == 0 else index_at(place - distance, n)
                at = pl.ds(number * tokens + first, count)
                total = (x_ref, w_ref)[number][dest, pl.ds(first, count)]
                if step > 0 and used(side, step - 1, part):
                    piece(side, step - 1, part).wait_recv()
                    total = (total.astype(jnp.float32) + recv_buf[side, step - 1, at].astype(jnp.float32)).astype(jnp.bfloat16)
                send_buf[side, step, at] = total
                copy = piece(side, step, part)
                copy.start()
                started.append(copy)
    for part, (number, first, count, _) in enumerate(parts):
        at = pl.ds(number * tokens + first, count)
        total = (x_ref, w_ref)[number][me, pl.ds(first, count)].astype(jnp.float32)
        for side in range(2):
            piece(side, hops - 1, part).wait_recv()
            total = total + recv_buf[side, hops - 1, at].astype(jnp.float32)
        (out_ref, gw_ref)[number][pl.ds(first, count)] = total
    for number in range(2):
        kept(number).wait()
        for away in range(1, tp):
            across(number, away).wait()
    for copy in started:
        copy.wait_send()


def ring_scatter(terms, weight_terms, keys, values, n, tp):
    rows, width = terms.shape[1:]
    rest = weight_terms.shape[1]
    hops = n // 2
    parts = ((0, 0, rows // 4, 0), (0, rows // 2, rows // 4, 1), (0, rows // 4, rows // 4, 0),
             (0, 3 * rows // 4, rows // 4, 1), (1, 0, rest // 2, 0), (1, rest // 2, rest // 2, 1))
    vmem = pl.BlockSpec(memory_space=pltpu.VMEM)
    own = jax.ShapeDtypeStruct((keys.shape[0] // tp, width * tp), jnp.bfloat16)
    return pl.pallas_call(
        functools.partial(scatter_kernel, n, tp, parts),
        out_shape=(
            jax.ShapeDtypeStruct((rows, width), jnp.float32),
            jax.ShapeDtypeStruct((rest, width), jnp.float32),
            own,
            own,
        ),
        in_specs=[vmem] * 4,
        out_specs=(vmem,) * 4,
        scratch_shapes=[
            pltpu.VMEM((2, hops, rows + rest, width), jnp.bfloat16),
            pltpu.VMEM((2, hops, rows + rest, width), jnp.bfloat16),
            pltpu.SemaphoreType.DMA((2, hops, len(parts))),
            pltpu.SemaphoreType.DMA((2, hops, len(parts))),
            pltpu.SemaphoreType.DMA((2, tp)),
            pltpu.SemaphoreType.DMA((2, tp)),
            pltpu.SemaphoreType.DMA((2,)),
        ],
        cost_estimate=pl.CostEstimate(flops=5 * 10**9, bytes_accessed=10**7, transcendentals=0),
        compiler_params=pltpu.CompilerParams(collective_id=1, has_side_effects=True, vmem_limit_bytes=50 << 20),
        name="ring_scatter",
    )(terms, weight_terms, keys, values)


NT = (((1,), (1,)), ((), ()))
TN = (((0,), (0,)), ((), ()))


def dot(left, right, dims=(((1,), (0,)), ((), ()))):
    return lax.dot_general(left, right, dims, preferred_element_type=jnp.float32)


def stats_kernel(blocks, heads, ids, q_ref, g_ref, k_ref, v_ref, out_ref):
    scale = HD ** (-0.5)
    block_len = q_ref.shape[1] // blocks

    @pl.loop(0, blocks)
    def _(block):
        picked = ids[pl.program_id(0) * blocks + block]

        @pl.when(picked < 0)
        def _():
            for head in range(heads):
                out_ref[block, 2 * head] = jnp.full((block_len,), FAR, jnp.float32)
                out_ref[block, 2 * head + 1] = jnp.zeros((block_len,), jnp.float32)

        @pl.when(picked >= 0)
        def _():
            tokens = pl.ds(pl.multiple_of(block * block_len, block_len), block_len)
            for head in range(heads):
                cols = pl.ds(head * HD, HD)
                scores = dot(k_ref[picked, :, cols], q_ref[0, tokens, cols], NT) * scale
                grads = dot(v_ref[picked, :, cols], g_ref[0, tokens, cols], NT)
                top = jnp.max(scores, axis=0, keepdims=True)
                raised = jnp.exp(scores - top)
                total = jnp.sum(raised, axis=0, keepdims=True)
                mean = jnp.sum(raised * grads, axis=0, keepdims=True) / total
                out_ref[block, pl.ds(2 * head, 1)] = top + jnp.log(total)
                out_ref[block, pl.ds(2 * head + 1, 1)] = mean


def grads_kernel(blocks, heads, ids, q_ref, g_ref, k_ref, v_ref, s_ref, dq_ref, pk_ref, pv_ref, dk_acc, dv_acc):
    scale = HD ** (-0.5)
    block_len = q_ref.shape[1] // blocks

    @pl.when(pl.program_id(0) == 0)
    def _():
        dk_acc[...] = jnp.zeros_like(dk_acc)
        dv_acc[...] = jnp.zeros_like(dv_acc)

    @pl.loop(0, blocks)
    def _(block):
        picked = ids[pl.program_id(0) * blocks + block]
        tokens = pl.ds(pl.multiple_of(block * block_len, block_len), block_len)

        @pl.when(picked < 0)
        def _():
            dq_ref[0, tokens] = jnp.zeros((block_len, heads * HD), jnp.bfloat16)

        @pl.when(picked >= 0)
        def _():
            for head in range(heads):
                cols = pl.ds(head * HD, HD)
                keys = k_ref[picked, :, cols]
                tok_q, tok_g = q_ref[0, tokens, cols], g_ref[0, tokens, cols]
                scores = dot(keys, tok_q, NT) * scale
                grads = dot(v_ref[picked, :, cols], tok_g, NT)
                weights = jnp.exp(scores - s_ref[block, pl.ds(2 * head, 1)])
                half = (weights * (grads - s_ref[block, pl.ds(2 * head + 1, 1)])).astype(jnp.bfloat16)
                dq_ref[0, tokens, cols] = (dot(half, keys, TN) * scale).astype(jnp.bfloat16)
                dk_acc[picked, :, cols] += dot(half, tok_q) * scale
                dv_acc[picked, :, cols] += dot(weights.astype(jnp.bfloat16), tok_g)

    @pl.when(pl.program_id(0) == pl.num_programs(0) - 1)
    def _():
        pk_ref[...] = dk_acc[...].astype(jnp.bfloat16)
        pv_ref[...] = dv_acc[...].astype(jnp.bfloat16)


def query_plan(queries, gate_pre, cotangent, store, store_gain, w_key, w_value, owners, slots):
    n = lax.axis_size("st")
    tp_size = lax.axis_size("tp")
    me = lax.axis_index("st")
    blocks, per_block = owners.shape
    tok_rows, local_width = queries.shape
    heads = local_width // HD
    block_len = tok_rows // blocks
    rows_dev = store.shape[0]
    passages = rows_dev // PLEN
    named = jnp.pad(owners * passages + slots, ((0, 0), (0, 128 - per_block)), constant_values=-1)
    gate_open = jax.nn.sigmoid(gate_pre.astype(jnp.float32))
    grad_in = (gate_open * cotangent.astype(jnp.float32)).astype(jnp.bfloat16)
    q_all, g_all, all_named = ring_gather(queries, grad_in, named, n)
    held = all_named.reshape(n * blocks, 128)[:, :per_block] - me * passages
    ids = jnp.max(jnp.where((held >= 0) & (held < passages), held, -1), axis=1)
    store_rows = store.astype(jnp.float32)
    row_inverse = row_scale(store_rows)
    normed = (store_rows * row_inverse * store_gain).astype(jnp.bfloat16)
    key_table = jnp.dot(normed, w_key, preferred_element_type=jnp.float32).astype(jnp.bfloat16)
    value_table = jnp.dot(normed, w_value, preferred_element_type=jnp.float32).astype(jnp.bfloat16)
    key_table = key_table.reshape(passages, PLEN, local_width)
    value_table = value_table.reshape(passages, PLEN, local_width)
    token_spec = pl.BlockSpec((1, tok_rows, local_width), lambda i, ids: (i, 0, 0))
    table_spec = pl.BlockSpec((passages, PLEN, local_width), lambda i, ids: (0, 0, 0))
    stat_spec = pl.BlockSpec((blocks, 2 * heads, block_len), lambda i, ids: (i, 0, 0))
    stats = pl.pallas_call(
        functools.partial(stats_kernel, blocks, heads),
        out_shape=jax.ShapeDtypeStruct((n * blocks, 2 * heads, block_len), jnp.float32),
        grid_spec=pltpu.PrefetchScalarGridSpec(
            num_scalar_prefetch=1,
            grid=(n,),
            in_specs=[token_spec, token_spec, table_spec, table_spec],
            out_specs=stat_spec,
        ),
        name="stats",
    )(ids, q_all, g_all, key_table, value_table)
    joined = join_stats(stats, n)
    dq, passage_keys, passage_values = pl.pallas_call(
        functools.partial(grads_kernel, blocks, heads),
        out_shape=(
            jax.ShapeDtypeStruct((n, tok_rows, local_width), jnp.bfloat16),
            jax.ShapeDtypeStruct((passages, PLEN, local_width), jnp.bfloat16),
            jax.ShapeDtypeStruct((passages, PLEN, local_width), jnp.bfloat16),
        ),
        grid_spec=pltpu.PrefetchScalarGridSpec(
            num_scalar_prefetch=1,
            grid=(n,),
            in_specs=[token_spec, token_spec, table_spec, table_spec, stat_spec],
            out_specs=(token_spec, table_spec, table_spec),
            scratch_shapes=[pltpu.VMEM((passages, PLEN, local_width), jnp.float32)] * 2,
        ),
        name="grads",
    )(ids, q_all, g_all, key_table, value_table, joined)
    passage_keys = passage_keys.reshape(rows_dev, local_width)
    passage_values = passage_values.reshape(rows_dev, local_width)
    weight_terms = lax.dot_general(
        normed, passage_values, (((0,), (0,)), ((), ())), preferred_element_type=jnp.float32
    ).astype(jnp.bfloat16)
    whole_key, whole_value = (
        lax.all_gather(w_key, "tp", axis=1, tiled=True),
        lax.all_gather(w_value, "tp", axis=1, tiled=True),
    )
    quarter = rows_dev // tp_size
    grad_queries, grad_w_value, own_keys, own_values = ring_scatter(
        dq, weight_terms.reshape(n, -1, local_width), passage_keys, passage_values, n, tp_size
    )
    grad_normed = contract(own_keys, whole_key) + contract(own_values, whole_value)
    first_row = lax.axis_index("tp") * quarter
    own_rows = lax.dynamic_slice_in_dim(store, first_row, quarter, 0).astype(jnp.float32)
    own_inverse = row_scale(own_rows)
    unit_rows = own_rows * own_inverse
    grad_unit = grad_normed * store_gain
    grad_store = own_inverse * (
        grad_unit - unit_rows * jnp.mean(grad_unit * unit_rows, axis=-1, keepdims=True)
    )
    return (grad_queries, grad_store, grad_w_value)


def local(*arrays):
    queries, owners = arrays[0], arrays[7]
    n = lax.axis_size("st")
    slot_cap = (2 * owners.size + n - 1) // n
    if n % 2 == 0 and n >= 4 and 8 * slot_cap * PLEN >= 3 * queries.shape[0]:
        return query_plan(*arrays)
    return passage_plan(*arrays)


def solution(mesh):
    placed = (
        P("st", "tp"),
        P("st", "tp"),
        P("st", "tp"),
        P("st", None),
        P(),
        P(None, "tp"),
        P(None, "tp"),
        P("st", None),
        P("st", None),
    )
    return jax.shard_map(
        local,
        mesh=mesh,
        in_specs=placed,
        out_specs=(P("st", "tp"), P(("st", "tp"), None), P("st", "tp")),
        check_vma=False,
    )
```

```python
import functools

import jax
import jax.numpy as jnp
from jax import lax
from jax.experimental import pallas as pl
from jax.experimental.pallas import tpu as pltpu
from jax.sharding import PartitionSpec as P

HD = 128
PLEN = 64


EPS = 1e-06


def row_scale(store_rows):
    return lax.rsqrt(jnp.mean(store_rows * store_rows, axis=-1, keepdims=True) + EPS)


def contract(left, right):
    return lax.dot_general(
        left, right, (((1,), (1,)), ((), ())), preferred_element_type=jnp.float32
    )


def passage_plan(queries, gate_pre, cotangent, store, store_gain, w_key, w_value, owners, slots):
    st_size = lax.axis_size("st")
    tp_size = lax.axis_size("tp")
    blocks, per_block = owners.shape
    tok_rows, local_width = queries.shape
    head_dim = HD
    local_heads = local_width // head_dim
    block_len = tok_rows // blocks
    passage_len = PLEN
    rows_dev = store.shape[0]
    passages = rows_dev // passage_len
    slot_count = blocks * per_block
    slot_cap = (2 * slot_count + st_size - 1) // st_size
    store_rows = store.astype(jnp.float32)
    row_inverse = row_scale(store_rows)
    normed = (store_rows * row_inverse * store_gain).astype(jnp.bfloat16)
    key_table = jnp.dot(normed, w_key, preferred_element_type=jnp.float32).astype(jnp.bfloat16)
    value_table = jnp.dot(normed, w_value, preferred_element_type=jnp.float32).astype(jnp.bfloat16)
    key_table = key_table.reshape(passages, passage_len, local_width)
    value_table = value_table.reshape(passages, passage_len, local_width)
    owner_flat = owners.reshape(slot_count)
    slot_flat = slots.reshape(slot_count)
    slot_order = jnp.arange(slot_count, dtype=jnp.int32)
    earlier_same = (owner_flat[:, None] == owner_flat[None, :]) & (
        slot_order[None, :] < slot_order[:, None]
    )
    slot_rank = jnp.sum(earlier_same.astype(jnp.int32), axis=1)
    position = owner_flat * slot_cap + slot_rank
    places = jnp.arange(st_size * slot_cap, dtype=jnp.int32)
    slot_hits = position[:, None] == places[None, :]
    requests = jnp.sum(jnp.where(slot_hits, slot_flat[:, None], 0), axis=0)
    requests = requests.reshape(st_size, slot_cap)
    asked_ids = lax.all_to_all(requests, "st", split_axis=0, concat_axis=0, tiled=True)
    asked_flat = asked_ids.reshape(-1)
    shape_out = asked_ids.shape + (passage_len, local_width)
    picked_keys = jnp.take(key_table, asked_flat, axis=0).reshape(shape_out)
    picked_values = jnp.take(value_table, asked_flat, axis=0).reshape(shape_out)
    sent_keys = lax.all_to_all(picked_keys, "st", split_axis=0, concat_axis=0, tiled=True)
    sent_values = lax.all_to_all(picked_values, "st", split_axis=0, concat_axis=0, tiled=True)
    got_keys, got_values, asked_ids = (sent_keys, sent_values, asked_ids)
    span = per_block * passage_len
    mine_keys = jnp.take(
        got_keys.reshape(st_size * slot_cap, passage_len, local_width), position, axis=0
    )
    mine_values = jnp.take(
        got_values.reshape(st_size * slot_cap, passage_len, local_width), position, axis=0
    )
    mine_keys = mine_keys.reshape(blocks, span, local_heads, head_dim)
    mine_values = mine_values.reshape(blocks, span, local_heads, head_dim)
    score_scale = head_dim ** (-0.5)
    query_blocks = queries.reshape(blocks, block_len, local_heads, head_dim)
    gate_open = jax.nn.sigmoid(gate_pre.astype(jnp.float32))
    grad_in = (gate_open * cotangent.astype(jnp.float32)).astype(jnp.bfloat16)
    grad_in = grad_in.reshape(blocks, block_len, local_heads, head_dim)
    scores = (
        jnp.einsum("bqhd,bkhd->bhqk", query_blocks, mine_keys, preferred_element_type=jnp.float32)
        * score_scale
    )
    shifted = scores - jnp.max(scores, axis=-1, keepdims=True)
    weights = jnp.exp(shifted)
    weights = weights / jnp.sum(weights, axis=-1, keepdims=True)
    weights_half = weights.astype(jnp.bfloat16)
    attended = jnp.einsum(
        "bhqk,bkhd->bqhd", weights_half, mine_values, preferred_element_type=jnp.float32
    )
    row_delta = jnp.sum(grad_in.astype(jnp.float32) * attended, axis=-1)
    grad_weights = jnp.einsum(
        "bqhd,bkhd->bhqk", grad_in, mine_values, preferred_element_type=jnp.float32
    )
    grad_scores = weights * (grad_weights - jnp.transpose(row_delta, (0, 2, 1))[..., None])
    grad_half = grad_scores.astype(jnp.bfloat16)
    grad_queries = (
        jnp.einsum("bhqk,bkhd->bqhd", grad_half, mine_keys, preferred_element_type=jnp.float32)
        * score_scale
    )
    grad_queries = grad_queries.reshape(tok_rows, local_width)
    grad_keys = (
        jnp.einsum("bhqk,bqhd->bkhd", grad_half, query_blocks, preferred_element_type=jnp.float32)
        * score_scale
    )
    grad_values = jnp.einsum(
        "bhqk,bqhd->bkhd", weights_half, grad_in, preferred_element_type=jnp.float32
    )
    grad_keys = grad_keys.reshape(slot_count, passage_len, local_width)
    grad_values = grad_values.reshape(slot_count, passage_len, local_width)
    empty_slots = jnp.zeros((st_size * slot_cap, passage_len, local_width), jnp.bfloat16)
    outgoing_keys = empty_slots.at[position].set(grad_keys.astype(jnp.bfloat16))
    outgoing_values = empty_slots.at[position].set(grad_values.astype(jnp.bfloat16))
    back_keys, back_values = (
        lax.all_to_all(outgoing_keys, "st", split_axis=0, concat_axis=0, tiled=True),
        lax.all_to_all(outgoing_values, "st", split_axis=0, concat_axis=0, tiled=True),
    )
    asked_flat = asked_ids.reshape(-1)
    owner_pick = (asked_flat[None, :] == jnp.arange(passages, dtype=jnp.int32)[:, None]).astype(
        jnp.bfloat16
    )
    passage_keys = jnp.dot(
        owner_pick,
        back_keys.reshape(st_size * slot_cap, passage_len * local_width),
        preferred_element_type=jnp.float32,
    )
    passage_values = jnp.dot(
        owner_pick,
        back_values.reshape(st_size * slot_cap, passage_len * local_width),
        preferred_element_type=jnp.float32,
    )
    passage_keys = passage_keys.astype(jnp.bfloat16).reshape(rows_dev, local_width)
    passage_values = passage_values.astype(jnp.bfloat16).reshape(rows_dev, local_width)
    weight_terms = lax.dot_general(
        normed, passage_values, (((0,), (0,)), ((), ())), preferred_element_type=jnp.float32
    )
    grad_w_value = lax.psum_scatter(weight_terms, "st", scatter_dimension=0, tiled=True)
    quarter = rows_dev // tp_size
    whole_key, whole_value = (
        lax.all_gather(w_key, "tp", axis=1, tiled=True),
        lax.all_gather(w_value, "tp", axis=1, tiled=True),
    )
    own_keys, own_values = (
        lax.all_to_all(passage_keys, "tp", split_axis=0, concat_axis=1, tiled=True),
        lax.all_to_all(passage_values, "tp", split_axis=0, concat_axis=1, tiled=True),
    )
    grad_normed = contract(own_keys, whole_key) + contract(own_values, whole_value)
    first_row = lax.axis_index("tp") * quarter
    own_rows = lax.dynamic_slice_in_dim(store_rows, first_row, quarter, 0)
    own_inverse = lax.dynamic_slice_in_dim(row_inverse, first_row, quarter, 0)
    unit_rows = own_rows * own_inverse
    grad_unit = grad_normed * store_gain
    grad_store = own_inverse * (
        grad_unit - unit_rows * jnp.mean(grad_unit * unit_rows, axis=-1, keepdims=True)
    )
    return (grad_queries, grad_store, grad_w_value)


FAR = -1e30
MESH = pl.DeviceIdType.MESH


def place_of(index, n):
    odd = index % 2
    return (1 - odd) * (index // 2) + odd * (n - 1 - index // 2)


def index_at(place, n):
    place = (place + 2 * n) % n
    back = place // (n // 2)
    return (1 - back) * (2 * place) + back * (2 * (n - 1 - place) + 1)


def greet(others):
    barrier = pltpu.get_barrier_semaphore()
    for axis, other in others:
        pl.semaphore_signal(barrier, inc=1, device_id={axis: other}, device_id_type=MESH)
    pl.semaphore_wait(barrier, len(others))


def gather_kernel(n, q_ref, g_ref, i_ref, q_all, g_all, i_all, send_sem, recv_sem, own_sem):
    me = lax.axis_index("st")
    place = place_of(me, n)
    right, left = index_at(place + 1, n), index_at(place - 1, n)
    half_rows = q_ref.shape[0] // 2
    pairs = ((q_ref, q_all), (g_ref, g_all), (i_ref, i_all))
    greet((("st", left), ("st", right)))
    own = []
    for number, (src, dst) in enumerate(pairs):
        copy = pltpu.make_async_copy(src, dst.at[me], own_sem.at[number])
        copy.start()
        own.append(copy)
    hops = n // 2
    parts = ((2, 0), (0, 0), (0, 1), (1, 0), (1, 1))

    def last_on(side, part):
        return parts[part][1] == side

    def piece(side, step, part):
        number, half = parts[part]
        src, dst = pairs[number]
        origin = index_at(place - step, n) if side == 0 else index_at(place + step, n)
        rows = pl.ds(0, i_ref.shape[0]) if number == 2 else pl.ds(half * half_rows, half_rows)
        return pltpu.make_async_remote_copy(
            src_ref=src.at[rows] if step == 0 else dst.at[origin, rows],
            dst_ref=dst.at[origin, rows],
            send_sem=send_sem.at[side, step, part],
            recv_sem=recv_sem.at[side, step, part],
            device_id={"st": right if side == 0 else left},
            device_id_type=MESH,
        )

    started = []
    for step in range(hops):
        for part in range(5):
            for side in range(2):
                if step < hops - 1 or last_on(side, part):
                    if step > 0:
                        piece(side, step - 1, part).wait_recv()
                    copy = piece(side, step, part)
                    copy.start()
                    started.append(copy)
    for part in range(5):
        for side in range(2):
            if not last_on(side, part):
                piece(side, hops - 2, part).wait_recv()
    for part in range(5):
        piece(parts[part][1], hops - 1, part).wait_recv()
    for copy in own:
        copy.wait()
    for copy in started:
        copy.wait_send()


def ring_gather(queries, grad_in, named, n):
    hops = n // 2
    vmem = pl.BlockSpec(memory_space=pltpu.VMEM)
    sources = (queries, grad_in, named)
    return pl.pallas_call(
        functools.partial(gather_kernel, n),
        out_shape=tuple(jax.ShapeDtypeStruct((n,) + x.shape, x.dtype) for x in sources),
        in_specs=[vmem] * 3,
        out_specs=(vmem,) * 3,
        scratch_shapes=[
            pltpu.SemaphoreType.DMA((2, hops, 5)),
            pltpu.SemaphoreType.DMA((2, hops, 5)),
            pltpu.SemaphoreType.DMA((3,)),
        ],
        cost_estimate=pl.CostEstimate(flops=10**10, bytes_accessed=10**7, transcendentals=0),
        compiler_params=pltpu.CompilerParams(collective_id=0, has_side_effects=True, vmem_limit_bytes=40 << 20),
        name="ring_gather",
    )(*sources)


def join_kernel(n, heads, x_ref, out_ref, got, mine, send_sem, recv_sem, own_sem):
    me = lax.axis_index("st")
    peers = [(me + away) % n for away in range(1, n)]
    greet([("st", peer) for peer in peers])

    def piece(phase, away):
        peer = (me + away) % n
        return pltpu.make_async_remote_copy(
            src_ref=x_ref.at[peer] if phase == 0 else mine,
            dst_ref=got.at[me] if phase == 0 else out_ref.at[me],
            send_sem=send_sem.at[phase, away],
            recv_sem=recv_sem.at[phase, away],
            device_id={"st": peer},
            device_id_type=MESH,
        )

    for away in range(1, n):
        piece(0, away).start()
    local = pltpu.make_async_copy(x_ref.at[me], got.at[me], own_sem.at[0])
    local.start()
    local.wait()
    for away in range(1, n):
        piece(0, away).wait()
    for head in range(heads):
        logs = [got[owner, :, 2 * head] for owner in range(n)]
        top = functools.reduce(jnp.maximum, logs)
        shares = [jnp.exp(one - top) for one in logs]
        total = sum(shares)
        mine[:, 2 * head] = top + jnp.log(total)
        mine[:, 2 * head + 1] = sum(share * got[owner, :, 2 * head + 1] for owner, share in enumerate(shares)) / total
    out_ref[me] = mine[...]
    for away in range(1, n):
        piece(1, away).start()
    for away in range(1, n):
        piece(1, away).wait()


def join_stats(stats, n):
    total, rows, width = stats.shape
    blocks = total // n
    vmem = pl.BlockSpec(memory_space=pltpu.VMEM)
    joined = pl.pallas_call(
        functools.partial(join_kernel, n, rows // 2),
        out_shape=jax.ShapeDtypeStruct((n, blocks, rows, width), jnp.float32),
        in_specs=[vmem],
        out_specs=vmem,
        scratch_shapes=[
            pltpu.VMEM((n, blocks, rows, width), jnp.float32),
            pltpu.VMEM((blocks, rows, width), jnp.float32),
            pltpu.SemaphoreType.DMA((2, n)),
            pltpu.SemaphoreType.DMA((2, n)),
            pltpu.SemaphoreType.DMA((1,)),
        ],
        cost_estimate=pl.CostEstimate(flops=10**9, bytes_accessed=10**6, transcendentals=0),
        compiler_params=pltpu.CompilerParams(collective_id=2, has_side_effects=True),
        name="join_stats",
    )(stats.reshape(n, blocks, rows, width))
    return joined.reshape(total, rows, width)


def scatter_kernel(n, tp, parts, x_ref, w_ref, k_ref, v_ref, out_ref, gw_ref, ok_ref, ov_ref, send_buf, recv_buf, send_sem, recv_sem, tp_send, tp_recv, own_sem):
    me = lax.axis_index("st")
    mine = lax.axis_index("tp")
    place = place_of(me, n)
    right, left = index_at(place + 1, n), index_at(place - 1, n)
    tokens = x_ref.shape[1]
    greet([("st", left), ("st", right)] + [("tp", (mine + away) % tp) for away in range(1, tp)])
    quarter, width = ok_ref.shape[0], k_ref.shape[1]
    columns = pl.ds(pl.multiple_of(mine * width, 128), width)

    def across(number, away):
        src, dst = ((k_ref, ok_ref), (v_ref, ov_ref))[number]
        peer = (mine + away) % tp
        return pltpu.make_async_remote_copy(
            src_ref=src.at[pl.ds(pl.multiple_of(peer * quarter, 16), quarter)],
            dst_ref=dst.at[:, columns],
            send_sem=tp_send.at[number, away],
            recv_sem=tp_recv.at[number, away],
            device_id={"tp": peer},
            device_id_type=MESH,
        )

    def kept(number):
        src, dst = ((k_ref, ok_ref), (v_ref, ov_ref))[number]
        return pltpu.make_async_copy(
            src.at[pl.ds(pl.multiple_of(mine * quarter, 16), quarter)], dst.at[:, columns], own_sem.at[number]
        )

    for number in range(2):
        kept(number).start()
        for away in range(1, tp):
            across(number, away).start()
    hops = n // 2

    def used(side, step, part):
        return step > 0 or parts[part][3] == side

    def piece(side, step, part):
        number, first, count, _ = parts[part]
        at = pl.ds(number * tokens + first, count)
        return pltpu.make_async_remote_copy(
            src_ref=send_buf.at[side, step, at],
            dst_ref=recv_buf.at[side, step, at],
            send_sem=send_sem.at[side, step, part],
            recv_sem=recv_sem.at[side, step, part],
            device_id={"st": right if side == 0 else left},
            device_id_type=MESH,
        )

    started = []
    for step in range(hops):
        for part, (number, first, count, _) in enumerate(parts):
            for side in range(2):
                if not used(side, step, part):
                    continue
                distance = hops - step
                dest = index_at(place + distance, n) if side == 0 else index_at(place - distance, n)
                at = pl.ds(number * tokens + first, count)
                total = (x_ref, w_ref)[number][dest, pl.ds(first, count)]
                if step > 0 and used(side, step - 1, part):
                    piece(side, step - 1, part).wait_recv()
                    total = (total.astype(jnp.float32) + recv_buf[side, step - 1, at].astype(jnp.float32)).astype(jnp.bfloat16)
                send_buf[side, step, at] = total
                copy = piece(side, step, part)
                copy.start()
                started.append(copy)
    for part, (number, first, count, _) in enumerate(parts):
        at = pl.ds(number * tokens + first, count)
        total = (x_ref, w_ref)[number][me, pl.ds(first, count)].astype(jnp.float32)
        for side in range(2):
            piece(side, hops - 1, part).wait_recv()
            total = total + recv_buf[side, hops - 1, at].astype(jnp.float32)
        (out_ref, gw_ref)[number][pl.ds(first, count)] = total
    for number in range(2):
        kept(number).wait()
        for away in range(1, tp):
            across(number, away).wait()
    for copy in started:
        copy.wait_send()


def ring_scatter(terms, weight_terms, keys, values, n, tp):
    rows, width = terms.shape[1:]
    rest = weight_terms.shape[1]
    hops = n // 2
    parts = ((0, 0, rows // 4, 0), (0, rows // 2, rows // 4, 1), (0, rows // 4, rows // 4, 0),
             (0, 3 * rows // 4, rows // 4, 1), (1, 0, rest // 2, 0), (1, rest // 2, rest // 2, 1))
    vmem = pl.BlockSpec(memory_space=pltpu.VMEM)
    own = jax.ShapeDtypeStruct((keys.shape[0] // tp, width * tp), jnp.bfloat16)
    return pl.pallas_call(
        functools.partial(scatter_kernel, n, tp, parts),
        out_shape=(
            jax.ShapeDtypeStruct((rows, width), jnp.float32),
            jax.ShapeDtypeStruct((rest, width), jnp.float32),
            own,
            own,
        ),
        in_specs=[vmem] * 4,
        out_specs=(vmem,) * 4,
        scratch_shapes=[
            pltpu.VMEM((2, hops, rows + rest, width), jnp.bfloat16),
            pltpu.VMEM((2, hops, rows + rest, width), jnp.bfloat16),
            pltpu.SemaphoreType.DMA((2, hops, len(parts))),
            pltpu.SemaphoreType.DMA((2, hops, len(parts))),
            pltpu.SemaphoreType.DMA((2, tp)),
            pltpu.SemaphoreType.DMA((2, tp)),
            pltpu.SemaphoreType.DMA((2,)),
        ],
        cost_estimate=pl.CostEstimate(flops=5 * 10**9, bytes_accessed=10**7, transcendentals=0),
        compiler_params=pltpu.CompilerParams(collective_id=1, has_side_effects=True, vmem_limit_bytes=50 << 20),
        name="ring_scatter",
    )(terms, weight_terms, keys, values)


NT = (((1,), (1,)), ((), ()))
TN = (((0,), (0,)), ((), ()))


def dot(left, right, dims=(((1,), (0,)), ((), ()))):
    return lax.dot_general(left, right, dims, preferred_element_type=jnp.float32)


def items_of(table, total, heads, turn):
    items = []
    for lane in range(2):
        block = table[total + 2 * turn + lane]
        picked = table[block]
        for head in range(heads):
            items.append((block, picked >= 0, jnp.maximum(picked, 0), head, pl.ds(head * HD, HD)))
    return items


def raw_products(items, q_ref, g_ref, k_ref, v_ref):
    scale = HD ** (-0.5)
    scores = [dot(k_ref[picked, :, cols], q_ref[block, :, cols], NT) * scale for block, _, picked, _, cols in items]
    grads = [dot(v_ref[picked, :, cols], g_ref[block, :, cols], NT) for block, _, picked, _, cols in items]
    return scores, grads


def stats_kernel(heads, table, q_ref, g_ref, k_ref, v_ref, out_ref):
    total, _, block_len = out_ref.shape

    @pl.loop(0, total)
    def _(block):
        for head in range(heads):
            out_ref[block, 2 * head] = jnp.full((block_len,), FAR, jnp.float32)
            out_ref[block, 2 * head + 1] = jnp.zeros((block_len,), jnp.float32)

    @pl.loop(0, (table[2 * total] + 1) // 2)
    def _(turn):
        items = items_of(table, total, heads, turn)
        scores, grads = raw_products(items, q_ref, g_ref, k_ref, v_ref)
        tops = [jnp.max(one, axis=0, keepdims=True) for one in scores]
        raised = [jnp.exp(one - top) for one, top in zip(scores, tops)]
        totals = [jnp.sum(one, axis=0, keepdims=True) for one in raised]
        means = [jnp.sum(one * two, axis=0, keepdims=True) / three for one, two, three in zip(raised, grads, totals)]
        logs = [top + jnp.log(one) for top, one in zip(tops, totals)]
        for number, (block, live, _, head, _) in enumerate(items):
            @pl.when(live)
            def _():
                out_ref[block, pl.ds(2 * head, 1)] = logs[number]
                out_ref[block, pl.ds(2 * head + 1, 1)] = means[number]


def grads_kernel(heads, table, q_ref, g_ref, k_ref, v_ref, s_ref, dq_ref, pk_ref, pv_ref, dk_acc, dv_acc):
    scale = HD ** (-0.5)
    total = dq_ref.shape[0]
    dk_acc[...] = jnp.zeros_like(dk_acc)
    dv_acc[...] = jnp.zeros_like(dv_acc)

    @pl.loop(table[2 * total], total)
    def _(at):
        dq_ref[table[total + at]] = jnp.zeros(dq_ref.shape[1:], jnp.bfloat16)

    @pl.loop(0, (table[2 * total] + 1) // 2)
    def _(turn):
        items = items_of(table, total, heads, turn)
        scores, grads = raw_products(items, q_ref, g_ref, k_ref, v_ref)
        weights, halves = [], []
        for (block, _, _, head, _), score, grad in zip(items, scores, grads):
            weight = jnp.exp(score - s_ref[block, pl.ds(2 * head, 1)])
            halves.append((weight * (grad - s_ref[block, pl.ds(2 * head + 1, 1)])).astype(jnp.bfloat16))
            weights.append(weight.astype(jnp.bfloat16))
        steps, keys, values = [], [], []
        for (block, _, picked, _, cols), weight, half in zip(items, weights, halves):
            keys.append(dot(half, q_ref[block, :, cols]) * scale)
            values.append(dot(weight, g_ref[block, :, cols]))
            steps.append((dot(half, k_ref[picked, :, cols], TN) * scale).astype(jnp.bfloat16))
        for number, (block, live, picked, _, cols) in enumerate(items):
            @pl.when(live)
            def _():
                dq_ref[block, :, cols] = steps[number]
                dk_acc[picked, :, cols] += keys[number]
                dv_acc[picked, :, cols] += values[number]

    pk_ref[...] = dk_acc[...].astype(jnp.bfloat16)
    pv_ref[...] = dv_acc[...].astype(jnp.bfloat16)


def table_of(ids):
    total = ids.shape[0]
    spot = jnp.arange(total, dtype=jnp.int32)
    idle = (ids < 0).astype(jnp.int32)
    sort_key = idle * total + spot
    rank = jnp.sum((sort_key[None, :] < sort_key[:, None]).astype(jnp.int32), axis=1)
    order = jnp.sum(jnp.where(rank[None, :] == spot[:, None], spot[None, :], 0), axis=1)
    count = total - jnp.sum(idle)
    return jnp.concatenate([ids, order, count[None]])


def query_plan(queries, gate_pre, cotangent, store, store_gain, w_key, w_value, owners, slots):
    n = lax.axis_size("st")
    tp_size = lax.axis_size("tp")
    me = lax.axis_index("st")
    blocks, per_block = owners.shape
    tok_rows, local_width = queries.shape
    heads = local_width // HD
    block_len = tok_rows // blocks
    rows_dev = store.shape[0]
    passages = rows_dev // PLEN
    named = jnp.pad(owners * passages + slots, ((0, 0), (0, 128 - per_block)), constant_values=-1)
    gate_open = jax.nn.sigmoid(gate_pre.astype(jnp.float32))
    grad_in = (gate_open * cotangent.astype(jnp.float32)).astype(jnp.bfloat16)
    q_all, g_all, all_named = ring_gather(queries, grad_in, named, n)
    held = all_named.reshape(n * blocks, 128)[:, :per_block] - me * passages
    ids = jnp.max(jnp.where((held >= 0) & (held < passages), held, -1), axis=1)
    store_rows = store.astype(jnp.float32)
    row_inverse = row_scale(store_rows)
    normed = (store_rows * row_inverse * store_gain).astype(jnp.bfloat16)
    key_table = jnp.dot(normed, w_key, preferred_element_type=jnp.float32).astype(jnp.bfloat16)
    value_table = jnp.dot(normed, w_value, preferred_element_type=jnp.float32).astype(jnp.bfloat16)
    key_table = key_table.reshape(passages, PLEN, local_width)
    value_table = value_table.reshape(passages, PLEN, local_width)
    table = table_of(ids)
    total = n * blocks
    q_blocks = q_all.reshape(total, block_len, local_width)
    g_blocks = g_all.reshape(total, block_len, local_width)
    smem = pl.BlockSpec(memory_space=pltpu.SMEM)
    vmem = pl.BlockSpec(memory_space=pltpu.VMEM)
    stats = pl.pallas_call(
        functools.partial(stats_kernel, heads),
        out_shape=jax.ShapeDtypeStruct((total, 2 * heads, block_len), jnp.float32),
        in_specs=[smem] + [vmem] * 4,
        out_specs=vmem,
        compiler_params=pltpu.CompilerParams(vmem_limit_bytes=40 << 20),
        name="stats",
    )(table, q_blocks, g_blocks, key_table, value_table)
    joined = join_stats(stats, n)
    dq, passage_keys, passage_values = pl.pallas_call(
        functools.partial(grads_kernel, heads),
        out_shape=(
            jax.ShapeDtypeStruct((total, block_len, local_width), jnp.bfloat16),
            jax.ShapeDtypeStruct((passages, PLEN, local_width), jnp.bfloat16),
            jax.ShapeDtypeStruct((passages, PLEN, local_width), jnp.bfloat16),
        ),
        in_specs=[smem] + [vmem] * 5,
        out_specs=(vmem,) * 3,
        scratch_shapes=[pltpu.VMEM((passages, PLEN, local_width), jnp.float32)] * 2,
        compiler_params=pltpu.CompilerParams(vmem_limit_bytes=40 << 20),
        name="grads",
    )(table, q_blocks, g_blocks, key_table, value_table, joined)
    dq = dq.reshape(n, tok_rows, local_width)
    passage_keys = passage_keys.reshape(rows_dev, local_width)
    passage_values = passage_values.reshape(rows_dev, local_width)
    weight_terms = lax.dot_general(
        normed, passage_values, (((0,), (0,)), ((), ())), preferred_element_type=jnp.float32
    ).astype(jnp.bfloat16)
    whole_key, whole_value = (
        lax.all_gather(w_key, "tp", axis=1, tiled=True),
        lax.all_gather(w_value, "tp", axis=1, tiled=True),
    )
    quarter = rows_dev // tp_size
    grad_queries, grad_w_value, own_keys, own_values = ring_scatter(
        dq, weight_terms.reshape(n, -1, local_width), passage_keys, passage_values, n, tp_size
    )
    grad_normed = contract(own_keys, whole_key) + contract(own_values, whole_value)
    first_row = lax.axis_index("tp") * quarter
    own_rows = lax.dynamic_slice_in_dim(store, first_row, quarter, 0).astype(jnp.float32)
    own_inverse = row_scale(own_rows)
    unit_rows = own_rows * own_inverse
    grad_unit = grad_normed * store_gain
    grad_store = own_inverse * (
        grad_unit - unit_rows * jnp.mean(grad_unit * unit_rows, axis=-1, keepdims=True)
    )
    return (grad_queries, grad_store, grad_w_value)


def local(*arrays):
    queries, owners = arrays[0], arrays[7]
    n = lax.axis_size("st")
    slot_cap = (2 * owners.size + n - 1) // n
    if n % 2 == 0 and n >= 4 and 8 * slot_cap * PLEN >= 3 * queries.shape[0]:
        return query_plan(*arrays)
    return passage_plan(*arrays)


def solution(mesh):
    placed = (
        P("st", "tp"),
        P("st", "tp"),
        P("st", "tp"),
        P("st", None),
        P(),
        P(None, "tp"),
        P(None, "tp"),
        P("st", None),
        P("st", None),
    )
    return jax.shard_map(
        local,
        mesh=mesh,
        in_specs=placed,
        out_specs=(P("st", "tp"), P(("st", "tp"), None), P("st", "tp")),
        check_vma=False,
    )
```

```python
import functools

import jax
import jax.numpy as jnp
from jax import lax
from jax.experimental import pallas as pl
from jax.experimental.pallas import tpu as pltpu
from jax.sharding import PartitionSpec as P

HD = 128
PLEN = 64


EPS = 1e-06


def row_scale(store_rows):
    return lax.rsqrt(jnp.mean(store_rows * store_rows, axis=-1, keepdims=True) + EPS)


def contract(left, right):
    return lax.dot_general(
        left, right, (((1,), (1,)), ((), ())), preferred_element_type=jnp.float32
    )


def passage_plan(queries, gate_pre, cotangent, store, store_gain, w_key, w_value, owners, slots):
    st_size = lax.axis_size("st")
    tp_size = lax.axis_size("tp")
    blocks, per_block = owners.shape
    tok_rows, local_width = queries.shape
    head_dim = HD
    local_heads = local_width // head_dim
    block_len = tok_rows // blocks
    passage_len = PLEN
    rows_dev = store.shape[0]
    passages = rows_dev // passage_len
    slot_count = blocks * per_block
    slot_cap = (2 * slot_count + st_size - 1) // st_size
    store_rows = store.astype(jnp.float32)
    row_inverse = row_scale(store_rows)
    normed = (store_rows * row_inverse * store_gain).astype(jnp.bfloat16)
    key_table = jnp.dot(normed, w_key, preferred_element_type=jnp.float32).astype(jnp.bfloat16)
    value_table = jnp.dot(normed, w_value, preferred_element_type=jnp.float32).astype(jnp.bfloat16)
    key_table = key_table.reshape(passages, passage_len, local_width)
    value_table = value_table.reshape(passages, passage_len, local_width)
    owner_flat = owners.reshape(slot_count)
    slot_flat = slots.reshape(slot_count)
    slot_order = jnp.arange(slot_count, dtype=jnp.int32)
    earlier_same = (owner_flat[:, None] == owner_flat[None, :]) & (
        slot_order[None, :] < slot_order[:, None]
    )
    slot_rank = jnp.sum(earlier_same.astype(jnp.int32), axis=1)
    position = owner_flat * slot_cap + slot_rank
    places = jnp.arange(st_size * slot_cap, dtype=jnp.int32)
    slot_hits = position[:, None] == places[None, :]
    requests = jnp.sum(jnp.where(slot_hits, slot_flat[:, None], 0), axis=0)
    requests = requests.reshape(st_size, slot_cap)
    asked_ids = lax.all_to_all(requests, "st", split_axis=0, concat_axis=0, tiled=True)
    asked_flat = asked_ids.reshape(-1)
    shape_out = asked_ids.shape + (passage_len, local_width)
    picked_keys = jnp.take(key_table, asked_flat, axis=0).reshape(shape_out)
    picked_values = jnp.take(value_table, asked_flat, axis=0).reshape(shape_out)
    sent_keys = lax.all_to_all(picked_keys, "st", split_axis=0, concat_axis=0, tiled=True)
    sent_values = lax.all_to_all(picked_values, "st", split_axis=0, concat_axis=0, tiled=True)
    got_keys, got_values, asked_ids = (sent_keys, sent_values, asked_ids)
    span = per_block * passage_len
    mine_keys = jnp.take(
        got_keys.reshape(st_size * slot_cap, passage_len, local_width), position, axis=0
    )
    mine_values = jnp.take(
        got_values.reshape(st_size * slot_cap, passage_len, local_width), position, axis=0
    )
    mine_keys = mine_keys.reshape(blocks, span, local_heads, head_dim)
    mine_values = mine_values.reshape(blocks, span, local_heads, head_dim)
    score_scale = head_dim ** (-0.5)
    query_blocks = queries.reshape(blocks, block_len, local_heads, head_dim)
    gate_open = jax.nn.sigmoid(gate_pre.astype(jnp.float32))
    grad_in = (gate_open * cotangent.astype(jnp.float32)).astype(jnp.bfloat16)
    grad_in = grad_in.reshape(blocks, block_len, local_heads, head_dim)
    scores = (
        jnp.einsum("bqhd,bkhd->bhqk", query_blocks, mine_keys, preferred_element_type=jnp.float32)
        * score_scale
    )
    shifted = scores - jnp.max(scores, axis=-1, keepdims=True)
    weights = jnp.exp(shifted)
    weights = weights / jnp.sum(weights, axis=-1, keepdims=True)
    weights_half = weights.astype(jnp.bfloat16)
    attended = jnp.einsum(
        "bhqk,bkhd->bqhd", weights_half, mine_values, preferred_element_type=jnp.float32
    )
    row_delta = jnp.sum(grad_in.astype(jnp.float32) * attended, axis=-1)
    grad_weights = jnp.einsum(
        "bqhd,bkhd->bhqk", grad_in, mine_values, preferred_element_type=jnp.float32
    )
    grad_scores = weights * (grad_weights - jnp.transpose(row_delta, (0, 2, 1))[..., None])
    grad_half = grad_scores.astype(jnp.bfloat16)
    grad_queries = (
        jnp.einsum("bhqk,bkhd->bqhd", grad_half, mine_keys, preferred_element_type=jnp.float32)
        * score_scale
    )
    grad_queries = grad_queries.reshape(tok_rows, local_width)
    grad_keys = (
        jnp.einsum("bhqk,bqhd->bkhd", grad_half, query_blocks, preferred_element_type=jnp.float32)
        * score_scale
    )
    grad_values = jnp.einsum(
        "bhqk,bqhd->bkhd", weights_half, grad_in, preferred_element_type=jnp.float32
    )
    grad_keys = grad_keys.reshape(slot_count, passage_len, local_width)
    grad_values = grad_values.reshape(slot_count, passage_len, local_width)
    empty_slots = jnp.zeros((st_size * slot_cap, passage_len, local_width), jnp.bfloat16)
    outgoing_keys = empty_slots.at[position].set(grad_keys.astype(jnp.bfloat16))
    outgoing_values = empty_slots.at[position].set(grad_values.astype(jnp.bfloat16))
    back_keys, back_values = (
        lax.all_to_all(outgoing_keys, "st", split_axis=0, concat_axis=0, tiled=True),
        lax.all_to_all(outgoing_values, "st", split_axis=0, concat_axis=0, tiled=True),
    )
    asked_flat = asked_ids.reshape(-1)
    owner_pick = (asked_flat[None, :] == jnp.arange(passages, dtype=jnp.int32)[:, None]).astype(
        jnp.bfloat16
    )
    passage_keys = jnp.dot(
        owner_pick,
        back_keys.reshape(st_size * slot_cap, passage_len * local_width),
        preferred_element_type=jnp.float32,
    )
    passage_values = jnp.dot(
        owner_pick,
        back_values.reshape(st_size * slot_cap, passage_len * local_width),
        preferred_element_type=jnp.float32,
    )
    passage_keys = passage_keys.astype(jnp.bfloat16).reshape(rows_dev, local_width)
    passage_values = passage_values.astype(jnp.bfloat16).reshape(rows_dev, local_width)
    weight_terms = lax.dot_general(
        normed, passage_values, (((0,), (0,)), ((), ())), preferred_element_type=jnp.float32
    )
    grad_w_value = lax.psum_scatter(weight_terms, "st", scatter_dimension=0, tiled=True)
    quarter = rows_dev // tp_size
    whole_key, whole_value = (
        lax.all_gather(w_key, "tp", axis=1, tiled=True),
        lax.all_gather(w_value, "tp", axis=1, tiled=True),
    )
    own_keys, own_values = (
        lax.all_to_all(passage_keys, "tp", split_axis=0, concat_axis=1, tiled=True),
        lax.all_to_all(passage_values, "tp", split_axis=0, concat_axis=1, tiled=True),
    )
    grad_normed = contract(own_keys, whole_key) + contract(own_values, whole_value)
    first_row = lax.axis_index("tp") * quarter
    own_rows = lax.dynamic_slice_in_dim(store_rows, first_row, quarter, 0)
    own_inverse = lax.dynamic_slice_in_dim(row_inverse, first_row, quarter, 0)
    unit_rows = own_rows * own_inverse
    grad_unit = grad_normed * store_gain
    grad_store = own_inverse * (
        grad_unit - unit_rows * jnp.mean(grad_unit * unit_rows, axis=-1, keepdims=True)
    )
    return (grad_queries, grad_store, grad_w_value)


FAR = -1e30
MESH = pl.DeviceIdType.MESH


def place_of(index, n):
    odd = index % 2
    return (1 - odd) * (index // 2) + odd * (n - 1 - index // 2)


def index_at(place, n):
    place = (place + 2 * n) % n
    back = place // (n // 2)
    return (1 - back) * (2 * place) + back * (2 * (n - 1 - place) + 1)


def greet(others):
    barrier = pltpu.get_barrier_semaphore()
    for axis, other in others:
        pl.semaphore_signal(barrier, inc=1, device_id={axis: other}, device_id_type=MESH)
    pl.semaphore_wait(barrier, len(others))


def gather_kernel(n, q_ref, g_ref, i_ref, x_ref, gain_ref, wk_ref, wv_ref, q_all, g_all, i_all, normed_ref, kt_ref, vt_ref, send_sem, recv_sem, own_sem):
    me = lax.axis_index("st")
    place = place_of(me, n)
    right, left = index_at(place + 1, n), index_at(place - 1, n)
    half_rows = q_ref.shape[0] // 2
    pairs = ((q_ref, q_all), (g_ref, g_all), (i_ref, i_all))
    greet((("st", left), ("st", right)))
    own = []
    for number, (src, dst) in enumerate(pairs):
        copy = pltpu.make_async_copy(src, dst.at[me], own_sem.at[number])
        copy.start()
        own.append(copy)
    hops = n // 2
    parts = ((2, 0), (0, 0), (0, 1), (1, 0), (1, 1))

    def last_on(side, part):
        return parts[part][1] == side

    def piece(side, step, part):
        number, half = parts[part]
        src, dst = pairs[number]
        origin = index_at(place - step, n) if side == 0 else index_at(place + step, n)
        rows = pl.ds(0, i_ref.shape[0]) if number == 2 else pl.ds(half * half_rows, half_rows)
        return pltpu.make_async_remote_copy(
            src_ref=src.at[rows] if step == 0 else dst.at[origin, rows],
            dst_ref=dst.at[origin, rows],
            send_sem=send_sem.at[side, step, part],
            recv_sem=recv_sem.at[side, step, part],
            device_id={"st": right if side == 0 else left},
            device_id_type=MESH,
        )

    count = x_ref.shape[0] // 128

    def project(chunk):
        rows = pl.ds(chunk * 128, 128)
        wide = x_ref[rows].astype(jnp.float32)
        normed = (wide * row_scale(wide) * gain_ref[...]).astype(jnp.bfloat16)
        normed_ref[rows] = normed
        kt_ref[rows] = jnp.dot(normed, wk_ref[...], preferred_element_type=jnp.float32).astype(jnp.bfloat16)
        vt_ref[rows] = jnp.dot(normed, wv_ref[...], preferred_element_type=jnp.float32).astype(jnp.bfloat16)

    chunk = 0
    started = []
    for step in range(hops):
        for part in range(5):
            for side in range(2):
                if step < hops - 1 or last_on(side, part):
                    if step > 0:
                        piece(side, step - 1, part).wait_recv()
                    copy = piece(side, step, part)
                    copy.start()
                    started.append(copy)
            if part > 0 and chunk < count:
                project(chunk)
                chunk += 1
    for rest in range(chunk, count):
        project(rest)
    for part in range(5):
        for side in range(2):
            if not last_on(side, part):
                piece(side, hops - 2, part).wait_recv()
    for part in range(5):
        piece(parts[part][1], hops - 1, part).wait_recv()
    for copy in own:
        copy.wait()
    for copy in started:
        copy.wait_send()


def ring_gather(queries, grad_in, named, store, gain, w_key, w_value, n):
    hops = n // 2
    vmem = pl.BlockSpec(memory_space=pltpu.VMEM)
    sources = (queries, grad_in, named)
    return pl.pallas_call(
        functools.partial(gather_kernel, n),
        out_shape=tuple(jax.ShapeDtypeStruct((n,) + x.shape, x.dtype) for x in sources)
        + (jax.ShapeDtypeStruct(store.shape, jnp.bfloat16),)
        + (jax.ShapeDtypeStruct((store.shape[0], w_key.shape[1]), jnp.bfloat16),) * 2,
        in_specs=[vmem] * 7,
        out_specs=(vmem,) * 6,
        scratch_shapes=[
            pltpu.SemaphoreType.DMA((2, hops, 5)),
            pltpu.SemaphoreType.DMA((2, hops, 5)),
            pltpu.SemaphoreType.DMA((3,)),
        ],
        cost_estimate=pl.CostEstimate(flops=10**10, bytes_accessed=10**7, transcendentals=0),
        compiler_params=pltpu.CompilerParams(collective_id=0, has_side_effects=True, vmem_limit_bytes=40 << 20),
        name="ring_gather",
    )(*sources, store, gain[None], w_key, w_value)


def join_kernel(n, heads, x_ref, out_ref, got, mine, send_sem, recv_sem, own_sem):
    me = lax.axis_index("st")
    peers = [(me + away) % n for away in range(1, n)]
    greet([("st", peer) for peer in peers])

    def piece(phase, away):
        peer = (me + away) % n
        return pltpu.make_async_remote_copy(
            src_ref=x_ref.at[peer] if phase == 0 else mine,
            dst_ref=got.at[me] if phase == 0 else out_ref.at[me],
            send_sem=send_sem.at[phase, away],
            recv_sem=recv_sem.at[phase, away],
            device_id={"st": peer},
            device_id_type=MESH,
        )

    for away in range(1, n):
        piece(0, away).start()
    local = pltpu.make_async_copy(x_ref.at[me], got.at[me], own_sem.at[0])
    local.start()
    local.wait()
    for away in range(1, n):
        piece(0, away).wait()
    for head in range(heads):
        logs = [got[owner, :, 2 * head] for owner in range(n)]
        top = functools.reduce(jnp.maximum, logs)
        shares = [jnp.exp(one - top) for one in logs]
        total = sum(shares)
        mine[:, 2 * head] = top + jnp.log(total)
        mine[:, 2 * head + 1] = sum(share * got[owner, :, 2 * head + 1] for owner, share in enumerate(shares)) / total
    out_ref[me] = mine[...]
    for away in range(1, n):
        piece(1, away).start()
    for away in range(1, n):
        piece(1, away).wait()


def join_stats(stats, n):
    total, rows, width = stats.shape
    blocks = total // n
    vmem = pl.BlockSpec(memory_space=pltpu.VMEM)
    joined = pl.pallas_call(
        functools.partial(join_kernel, n, rows // 2),
        out_shape=jax.ShapeDtypeStruct((n, blocks, rows, width), jnp.float32),
        in_specs=[vmem],
        out_specs=vmem,
        scratch_shapes=[
            pltpu.VMEM((n, blocks, rows, width), jnp.float32),
            pltpu.VMEM((blocks, rows, width), jnp.float32),
            pltpu.SemaphoreType.DMA((2, n)),
            pltpu.SemaphoreType.DMA((2, n)),
            pltpu.SemaphoreType.DMA((1,)),
        ],
        cost_estimate=pl.CostEstimate(flops=10**9, bytes_accessed=10**6, transcendentals=0),
        compiler_params=pltpu.CompilerParams(collective_id=2, has_side_effects=True),
        name="join_stats",
    )(stats.reshape(n, blocks, rows, width))
    return joined.reshape(total, rows, width)


def scatter_kernel(n, tp, parts, x_ref, w_ref, k_ref, v_ref, out_ref, gw_ref, ok_ref, ov_ref, send_buf, recv_buf, send_sem, recv_sem, tp_send, tp_recv, own_sem):
    me = lax.axis_index("st")
    mine = lax.axis_index("tp")
    place = place_of(me, n)
    right, left = index_at(place + 1, n), index_at(place - 1, n)
    tokens = x_ref.shape[1]
    greet([("st", left), ("st", right)] + [("tp", (mine + away) % tp) for away in range(1, tp)])
    quarter, width = ok_ref.shape[0], k_ref.shape[1]
    columns = pl.ds(pl.multiple_of(mine * width, 128), width)

    def across(number, away):
        src, dst = ((k_ref, ok_ref), (v_ref, ov_ref))[number]
        peer = (mine + away) % tp
        return pltpu.make_async_remote_copy(
            src_ref=src.at[pl.ds(pl.multiple_of(peer * quarter, 16), quarter)],
            dst_ref=dst.at[:, columns],
            send_sem=tp_send.at[number, away],
            recv_sem=tp_recv.at[number, away],
            device_id={"tp": peer},
            device_id_type=MESH,
        )

    def kept(number):
        src, dst = ((k_ref, ok_ref), (v_ref, ov_ref))[number]
        return pltpu.make_async_copy(
            src.at[pl.ds(pl.multiple_of(mine * quarter, 16), quarter)], dst.at[:, columns], own_sem.at[number]
        )

    for number in range(2):
        kept(number).start()
        for away in range(1, tp):
            across(number, away).start()
    hops = n // 2

    def used(side, step, part):
        return step > 0 or parts[part][3] == side

    def piece(side, step, part):
        number, first, count, _ = parts[part]
        at = pl.ds(number * tokens + first, count)
        return pltpu.make_async_remote_copy(
            src_ref=send_buf.at[side, step, at],
            dst_ref=recv_buf.at[side, step, at],
            send_sem=send_sem.at[side, step, part],
            recv_sem=recv_sem.at[side, step, part],
            device_id={"st": right if side == 0 else left},
            device_id_type=MESH,
        )

    started = []
    for step in range(hops):
        for part, (number, first, count, _) in enumerate(parts):
            for side in range(2):
                if not used(side, step, part):
                    continue
                distance = hops - step
                dest = index_at(place + distance, n) if side == 0 else index_at(place - distance, n)
                at = pl.ds(number * tokens + first, count)
                total = (x_ref, w_ref)[number][dest, pl.ds(first, count)]
                if step > 0 and used(side, step - 1, part):
                    piece(side, step - 1, part).wait_recv()
                    total = (total.astype(jnp.float32) + recv_buf[side, step - 1, at].astype(jnp.float32)).astype(jnp.bfloat16)
                send_buf[side, step, at] = total
                copy = piece(side, step, part)
                copy.start()
                started.append(copy)
    for part, (number, first, count, _) in enumerate(parts):
        at = pl.ds(number * tokens + first, count)
        total = (x_ref, w_ref)[number][me, pl.ds(first, count)].astype(jnp.float32)
        for side in range(2):
            piece(side, hops - 1, part).wait_recv()
            total = total + recv_buf[side, hops - 1, at].astype(jnp.float32)
        (out_ref, gw_ref)[number][pl.ds(first, count)] = total
    for number in range(2):
        kept(number).wait()
        for away in range(1, tp):
            across(number, away).wait()
    for copy in started:
        copy.wait_send()


def ring_scatter(terms, weight_terms, keys, values, n, tp):
    rows, width = terms.shape[1:]
    rest = weight_terms.shape[1]
    hops = n // 2
    parts = ((0, 0, rows // 4, 0), (0, rows // 2, rows // 4, 1), (0, rows // 4, rows // 4, 0),
             (0, 3 * rows // 4, rows // 4, 1), (1, 0, rest // 2, 0), (1, rest // 2, rest // 2, 1))
    vmem = pl.BlockSpec(memory_space=pltpu.VMEM)
    own = jax.ShapeDtypeStruct((keys.shape[0] // tp, width * tp), jnp.bfloat16)
    return pl.pallas_call(
        functools.partial(scatter_kernel, n, tp, parts),
        out_shape=(
            jax.ShapeDtypeStruct((rows, width), jnp.float32),
            jax.ShapeDtypeStruct((rest, width), jnp.float32),
            own,
            own,
        ),
        in_specs=[vmem] * 4,
        out_specs=(vmem,) * 4,
        scratch_shapes=[
            pltpu.VMEM((2, hops, rows + rest, width), jnp.bfloat16),
            pltpu.VMEM((2, hops, rows + rest, width), jnp.bfloat16),
            pltpu.SemaphoreType.DMA((2, hops, len(parts))),
            pltpu.SemaphoreType.DMA((2, hops, len(parts))),
            pltpu.SemaphoreType.DMA((2, tp)),
            pltpu.SemaphoreType.DMA((2, tp)),
            pltpu.SemaphoreType.DMA((2,)),
        ],
        cost_estimate=pl.CostEstimate(flops=5 * 10**9, bytes_accessed=10**7, transcendentals=0),
        compiler_params=pltpu.CompilerParams(collective_id=1, has_side_effects=True, vmem_limit_bytes=50 << 20),
        name="ring_scatter",
    )(terms, weight_terms, keys, values)


NT = (((1,), (1,)), ((), ()))
TN = (((0,), (0,)), ((), ()))


def dot(left, right, dims=(((1,), (0,)), ((), ()))):
    return lax.dot_general(left, right, dims, preferred_element_type=jnp.float32)


def items_of(table, total, heads, turn):
    items = []
    for lane in range(2):
        block = table[total + 2 * turn + lane]
        picked = table[block]
        for head in range(heads):
            items.append((block, picked >= 0, jnp.maximum(picked, 0), head, pl.ds(head * HD, HD)))
    return items


def raw_products(items, q_ref, g_ref, k_ref, v_ref):
    scale = HD ** (-0.5)
    scores = [dot(k_ref[picked, :, cols], q_ref[block, :, cols], NT) * scale for block, _, picked, _, cols in items]
    grads = [dot(v_ref[picked, :, cols], g_ref[block, :, cols], NT) for block, _, picked, _, cols in items]
    return scores, grads


def stats_kernel(heads, table, q_ref, g_ref, k_ref, v_ref, out_ref):
    total, _, block_len = out_ref.shape

    @pl.loop(0, total)
    def _(block):
        for head in range(heads):
            out_ref[block, 2 * head] = jnp.full((block_len,), FAR, jnp.float32)
            out_ref[block, 2 * head + 1] = jnp.zeros((block_len,), jnp.float32)

    @pl.loop(0, (table[2 * total] + 1) // 2)
    def _(turn):
        items = items_of(table, total, heads, turn)
        scores, grads = raw_products(items, q_ref, g_ref, k_ref, v_ref)
        tops = [jnp.max(one, axis=0, keepdims=True) for one in scores]
        raised = [jnp.exp(one - top) for one, top in zip(scores, tops)]
        totals = [jnp.sum(one, axis=0, keepdims=True) for one in raised]
        means = [jnp.sum(one * two, axis=0, keepdims=True) / three for one, two, three in zip(raised, grads, totals)]
        logs = [top + jnp.log(one) for top, one in zip(tops, totals)]
        for number, (block, live, _, head, _) in enumerate(items):
            @pl.when(live)
            def _():
                out_ref[block, pl.ds(2 * head, 1)] = logs[number]
                out_ref[block, pl.ds(2 * head + 1, 1)] = means[number]


def grads_kernel(heads, table, q_ref, g_ref, k_ref, v_ref, s_ref, dq_ref, pk_ref, pv_ref, dk_acc, dv_acc):
    scale = HD ** (-0.5)
    total = dq_ref.shape[0]
    dk_acc[...] = jnp.zeros_like(dk_acc)
    dv_acc[...] = jnp.zeros_like(dv_acc)

    @pl.loop(table[2 * total], total)
    def _(at):
        dq_ref[table[total + at]] = jnp.zeros(dq_ref.shape[1:], jnp.bfloat16)

    @pl.loop(0, (table[2 * total] + 1) // 2)
    def _(turn):
        items = items_of(table, total, heads, turn)
        scores, grads = raw_products(items, q_ref, g_ref, k_ref, v_ref)
        weights, halves = [], []
        for (block, _, _, head, _), score, grad in zip(items, scores, grads):
            weight = jnp.exp(score - s_ref[block, pl.ds(2 * head, 1)])
            halves.append((weight * (grad - s_ref[block, pl.ds(2 * head + 1, 1)])).astype(jnp.bfloat16))
            weights.append(weight.astype(jnp.bfloat16))
        steps, keys, values = [], [], []
        for (block, _, picked, _, cols), weight, half in zip(items, weights, halves):
            keys.append(dot(half, q_ref[block, :, cols]) * scale)
            values.append(dot(weight, g_ref[block, :, cols]))
            steps.append((dot(half, k_ref[picked, :, cols], TN) * scale).astype(jnp.bfloat16))
        for number, (block, live, picked, _, cols) in enumerate(items):
            @pl.when(live)
            def _():
                dq_ref[block, :, cols] = steps[number]
                dk_acc[picked, :, cols] += keys[number]
                dv_acc[picked, :, cols] += values[number]

    pk_ref[...] = dk_acc[...].astype(jnp.bfloat16)
    pv_ref[...] = dv_acc[...].astype(jnp.bfloat16)


def table_of(ids):
    total = ids.shape[0]
    spot = jnp.arange(total, dtype=jnp.int32)
    idle = (ids < 0).astype(jnp.int32)
    sort_key = idle * total + spot
    rank = jnp.sum((sort_key[None, :] < sort_key[:, None]).astype(jnp.int32), axis=1)
    order = jnp.sum(jnp.where(rank[None, :] == spot[:, None], spot[None, :], 0), axis=1)
    count = total - jnp.sum(idle)
    return jnp.concatenate([ids, order, count[None]])


def query_plan(queries, gate_pre, cotangent, store, store_gain, w_key, w_value, owners, slots):
    n = lax.axis_size("st")
    tp_size = lax.axis_size("tp")
    me = lax.axis_index("st")
    blocks, per_block = owners.shape
    tok_rows, local_width = queries.shape
    heads = local_width // HD
    block_len = tok_rows // blocks
    rows_dev = store.shape[0]
    passages = rows_dev // PLEN
    named = jnp.pad(owners * passages + slots, ((0, 0), (0, 128 - per_block)), constant_values=-1)
    gate_open = jax.nn.sigmoid(gate_pre.astype(jnp.float32))
    grad_in = (gate_open * cotangent.astype(jnp.float32)).astype(jnp.bfloat16)
    q_all, g_all, all_named, normed, key_table, value_table = ring_gather(
        queries, grad_in, named, store, store_gain, w_key, w_value, n
    )
    held = all_named.reshape(n * blocks, 128)[:, :per_block] - me * passages
    ids = jnp.max(jnp.where((held >= 0) & (held < passages), held, -1), axis=1)
    key_table = key_table.reshape(passages, PLEN, local_width)
    value_table = value_table.reshape(passages, PLEN, local_width)
    table = table_of(ids)
    total = n * blocks
    q_blocks = q_all.reshape(total, block_len, local_width)
    g_blocks = g_all.reshape(total, block_len, local_width)
    smem = pl.BlockSpec(memory_space=pltpu.SMEM)
    vmem = pl.BlockSpec(memory_space=pltpu.VMEM)
    stats = pl.pallas_call(
        functools.partial(stats_kernel, heads),
        out_shape=jax.ShapeDtypeStruct((total, 2 * heads, block_len), jnp.float32),
        in_specs=[smem] + [vmem] * 4,
        out_specs=vmem,
        compiler_params=pltpu.CompilerParams(vmem_limit_bytes=40 << 20),
        name="stats",
    )(table, q_blocks, g_blocks, key_table, value_table)
    joined = join_stats(stats, n)
    dq, passage_keys, passage_values = pl.pallas_call(
        functools.partial(grads_kernel, heads),
        out_shape=(
            jax.ShapeDtypeStruct((total, block_len, local_width), jnp.bfloat16),
            jax.ShapeDtypeStruct((passages, PLEN, local_width), jnp.bfloat16),
            jax.ShapeDtypeStruct((passages, PLEN, local_width), jnp.bfloat16),
        ),
        in_specs=[smem] + [vmem] * 5,
        out_specs=(vmem,) * 3,
        scratch_shapes=[pltpu.VMEM((passages, PLEN, local_width), jnp.float32)] * 2,
        compiler_params=pltpu.CompilerParams(vmem_limit_bytes=40 << 20),
        name="grads",
    )(table, q_blocks, g_blocks, key_table, value_table, joined)
    dq = dq.reshape(n, tok_rows, local_width)
    passage_keys = passage_keys.reshape(rows_dev, local_width)
    passage_values = passage_values.reshape(rows_dev, local_width)
    weight_terms = lax.dot_general(
        normed, passage_values, (((0,), (0,)), ((), ())), preferred_element_type=jnp.float32
    ).astype(jnp.bfloat16)
    whole_key, whole_value = (
        lax.all_gather(w_key, "tp", axis=1, tiled=True),
        lax.all_gather(w_value, "tp", axis=1, tiled=True),
    )
    quarter = rows_dev // tp_size
    grad_queries, grad_w_value, own_keys, own_values = ring_scatter(
        dq, weight_terms.reshape(n, -1, local_width), passage_keys, passage_values, n, tp_size
    )
    grad_normed = contract(own_keys, whole_key) + contract(own_values, whole_value)
    first_row = lax.axis_index("tp") * quarter
    own_rows = lax.dynamic_slice_in_dim(store, first_row, quarter, 0).astype(jnp.float32)
    own_inverse = row_scale(own_rows)
    unit_rows = own_rows * own_inverse
    grad_unit = grad_normed * store_gain
    grad_store = own_inverse * (
        grad_unit - unit_rows * jnp.mean(grad_unit * unit_rows, axis=-1, keepdims=True)
    )
    return (grad_queries, grad_store, grad_w_value)


def local(*arrays):
    queries, owners = arrays[0], arrays[7]
    n = lax.axis_size("st")
    slot_cap = (2 * owners.size + n - 1) // n
    if n % 2 == 0 and n >= 4 and 8 * slot_cap * PLEN >= 3 * queries.shape[0]:
        return query_plan(*arrays)
    return passage_plan(*arrays)


def solution(mesh):
    placed = (
        P("st", "tp"),
        P("st", "tp"),
        P("st", "tp"),
        P("st", None),
        P(),
        P(None, "tp"),
        P(None, "tp"),
        P("st", None),
        P("st", None),
    )
    return jax.shard_map(
        local,
        mesh=mesh,
        in_specs=placed,
        out_specs=(P("st", "tp"), P(("st", "tp"), None), P("st", "tp")),
        check_vma=False,
    )
```
